512 devices in a mesh: tp: 32 (over z, x), dp: 16 (over y, core).
Axes of the slice: x: 4, y: 8, z: 8, core: 2. Of those that a mesh axis runs over, the one named last changes fastest.
Arguments:
- tokens: bfloat16 [256, 4096], P(None, 'dp'), may hold values from -6 to 6
- recurrent_state: float32 [2, 256, 262144], P(None, 'dp', 'tp'), may hold values from -24 to 24
- pre_gain: float32 [2, 4096], P(None, 'dp'), may hold values from 0.1 to 1.9
- w_query: bfloat16 [2, 4096, 2048], P(None, 'dp', 'tp'), may hold values from -0.09375 to 0.09375
- w_key: bfloat16 [2, 4096, 2048], P(None, 'dp', 'tp'), may hold values from -0.09375 to 0.09375
- w_value: bfloat16 [2, 4096, 4096], P(None, 'dp', 'tp'), may hold values from -0.09375 to 0.09375
- w_gate: bfloat16 [2, 4096, 4096], P(None, 'dp', 'tp'), may hold values from -0.09375 to 0.09375
- w_decay: bfloat16 [2, 4096, 2048], P(None, 'dp', 'tp'), may hold values from -1 to 1
- decay_bias: float32 [2, 2048], P(None, 'tp'), may hold values from -5 to 3
- head_gain: float32 [2, 128], replicated, may hold values from 0.1 to 1.9
- w_out: bfloat16 [2, 4096, 4096], P(None, 'tp', 'dp'), may hold values from -0.09375 to 0.09375
- post_gain: float32 [2, 4096], P(None, 'dp'), may hold values from 0.1 to 1.9
Outputs:
- hidden_out: bfloat16 [256, 4096], P(None, 'dp')
- state_out: float32 [2, 256, 262144], P(None, 'dp', 'tp')
The draws below stay inside these ranges and needn't reach their ends.
All inputs are finite; a program needn't handle non-finite values.
Results may differ from the reference program's by a relative error of at most 0.015.
Values may be sent and summed in bfloat16 or wider, within the bound.
No kernel may reach another device: no remote copies, remote signals or barrier semaphores. Data moves between devices by JAX's collectives and lax.ppermute only.
A program may use at most 64 MiB of HBM per device.

```python
import jax
import jax.numpy as jnp
from jax import lax

D = 4096
HEADS = 32
KEY = 64
VAL = 128
QK = 2048
VW = 4096
SEQS = 256


def draw_recurrent_state(key, part):
    shape = (2, SEQS, VW * KEY)
    column = jnp.arange(VW * KEY, dtype=jnp.int32) // KEY
    within = (column % VAL).astype(jnp.float32) / (VAL - 1)
    ratio = 6.0
    noise = jnp.clip(jax.random.normal(key, shape, jnp.float32), -4.0, 4.0)
    scale = 0.5 * jnp.exp(jnp.log(ratio) * within)
    return (noise * scale[None, None, :]).astype(jnp.float32)


def levels(key, shape, split, smallest, high):
    level = 1.0
    for axis_at, blocks in split:
        heights = jax.random.uniform(jax.random.fold_in(jax.random.fold_in(key, 6), axis_at), (blocks,), jnp.float32, smallest / len(split), high / len(split))
        level = level * jnp.repeat(jnp.exp(heights), shape[axis_at] // blocks).reshape((-1,) + (1,) * (len(shape) - 1 - axis_at))
    return level


def scatter_about(key, shape, scale, reach, cuts=(), kind=jnp.bfloat16):
    values = jax.random.normal(key, shape, jnp.float32) * scale
    if len(cuts) > 0:
        values = levels(key, shape, cuts, -0.22, 0.18) * values
    return jnp.clip(values, min=-reach, max=reach).astype(kind)


def setup_inputs(seed: int = 0) -> dict:
    key_of = jax.random.split(jax.random.key(seed), 13)
    return {
        "tokens": scatter_about(key_of[0], (SEQS, D), 1.0, 6.0, ((1, 16),)),
        "recurrent_state": draw_recurrent_state(jax.random.fold_in(key_of[12], 71), 0),
        "pre_gain": jnp.clip(1.0 + 0.18 * jax.random.normal(key_of[2], (2, D), jnp.float32), 0.1, 1.9),
        "w_query": scatter_about(key_of[3], (2, D, QK), D ** -0.5, 0.09375, ((1, 16), (2, 32))),
        "w_key": scatter_about(key_of[4], (2, D, QK), D ** -0.5, 0.09375, ((1, 16), (2, 32))),
        "w_value": scatter_about(key_of[5], (2, D, VW), D ** -0.5, 0.09375, ((1, 16), (2, 32))),
        "w_gate": scatter_about(key_of[6], (2, D, VW), D ** -0.5, 0.09375, ((1, 16), (2, 32))),
        "w_decay": scatter_about(key_of[7], (2, D, QK), 0.0625, 1.0, ((1, 16), (2, 32))),
        "decay_bias": jnp.clip(-5.0 + 8.0 * jax.random.uniform(key_of[8], (2, QK), jnp.float32) ** levels(key_of[8], (2, QK), ((1, 32),), -0.2, 0.2), -5.0, 3.0),
        "head_gain": jnp.clip(1.0 + 0.18 * jax.random.normal(key_of[9], (2, VAL), jnp.float32), 0.1, 1.9),
        "w_out": scatter_about(key_of[10], (2, VW, D), VW ** -0.5, 0.09375, ((1, 32), (2, 16))),
        "post_gain": jnp.clip(1.0 + 0.18 * jax.random.normal(key_of[11], (2, D), jnp.float32), 0.1, 1.9),
    }


epsilon = 1e-06

def reference(tokens, recurrent_state, pre_gain, w_query, w_key, w_value, w_gate, w_decay, decay_bias, head_gain, w_out, post_gain):
    residual = tokens
    new_states = []
    for section_index in range(2):
        wide_float = residual.astype(jnp.float32)
        row_scale = lax.rsqrt(lax.optimization_barrier(jnp.mean(wide_float * wide_float, axis=1, keepdims=True)) + epsilon)
        normed = (wide_float * pre_gain[section_index]).astype(jnp.bfloat16)

        def project_role(weights):
            return jnp.dot(normed, weights[section_index], preferred_element_type=jnp.float32) * row_scale
        query = lax.optimization_barrier(project_role(w_query).astype(jnp.bfloat16)).astype(jnp.float32)
        key_vec = lax.optimization_barrier(project_role(w_key).astype(jnp.bfloat16)).astype(jnp.float32)
        values_own = project_role(w_value)
        gate_pre = project_role(w_gate)
        log_decay = jax.nn.log_sigmoid(project_role(w_decay) + decay_bias[section_index]) / 16.0
        seq_count = residual.shape[0]
        query = query.reshape(seq_count, HEADS, 1, KEY)
        key_vec = key_vec.reshape(seq_count, HEADS, 1, KEY)
        decay_rate = jnp.exp(log_decay).reshape(seq_count, HEADS, 1, KEY)
        old_state = recurrent_state[section_index].reshape(seq_count, HEADS, VAL, KEY)
        new_state = decay_rate * old_state + key_vec * values_own.reshape(seq_count, HEADS, VAL, 1)
        readout = lax.optimization_barrier(jnp.sum(query * new_state, axis=3)) * KEY ** (-0.5)
        head_mean = lax.optimization_barrier(jnp.mean(readout * readout, axis=-1, keepdims=True))
        mixed = readout * lax.rsqrt(head_mean + epsilon) * head_gain[section_index] * jax.nn.silu(gate_pre.reshape(seq_count, HEADS, VAL))
        mixed = mixed.reshape(seq_count, HEADS * VAL).astype(jnp.bfloat16)
        out_rows = jnp.dot(mixed, w_out[section_index], preferred_element_type=jnp.float32)
        out_scale = lax.rsqrt(lax.optimization_barrier(jnp.mean(out_rows * out_rows, axis=1, keepdims=True)) + epsilon)
        residual = (wide_float + out_rows * out_scale * post_gain[section_index]).astype(jnp.bfloat16)
        new_states.append(new_state.reshape(seq_count, HEADS * VAL * KEY))
    return (residual, jnp.stack(new_states))
```

```python
import functools

import jax
import jax.numpy as jnp
from jax import lax
from jax.experimental import pallas as pl
from jax.experimental.pallas import tpu as pltpu
from jax.sharding import PartitionSpec as P


D = 4096
KEY = 64
VAL = 128
DP = 16
TP = 32
LS = 16
epsilon = 1e-06
bf16 = jnp.bfloat16
f32 = jnp.float32

SWAP = [(d, d ^ 1) for d in range(DP)]
RING = [(2 * y, 2 * ((y + 1) % 8)) for y in range(8)] + [
    (2 * y + 1, 2 * ((y + 7) % 8) + 1) for y in range(8)
]


def whole(shape, index=None):
    at = index or (0,) * len(shape)
    return pl.BlockSpec(shape, lambda i, at=at: at)


def call(body, out_shape, in_specs, out_specs, scratch=(), aliases=None):
    return pl.pallas_call(
        body,
        grid=(1,),
        out_shape=out_shape,
        in_specs=in_specs,
        out_specs=out_specs,
        scratch_shapes=scratch,
        input_output_aliases=aliases or {},
    )


def owners():
    me = lax.axis_index("dp")
    y = me // 2
    c = me % 2
    sign = 2 * c - 1
    found = []
    for p in range(8):
        if p == 0:
            at, order = y, c
        elif p <= 4:
            at, order = (y + sign * p + 8) % 8, c
        else:
            at, order = (y - sign * (p - 4) + 8) % 8, 1 - c
        found.append((2 * at + order, 2 * at + 1 - order))
    return found


def columns(wq, wk, wv, wg, wd):
    qk = jnp.concatenate([wq[0], wk[0]], axis=0).astype(f32).T.astype(bf16)
    decay = jnp.concatenate([wd[0].astype(f32), jnp.zeros((64, 256), f32)], axis=0).T.astype(bf16)
    return (qk, wv[0], wg[0], decay)


def second_weights_body(wq, wk, wv, wg, wd, wo, out):
    for i, w in enumerate(columns(wq, wk, wv, wg, wd)):
        out[0:256, 128 * i : 128 * i + 128] = w
    out[256:320, 0:256] = wo[0, 0:64, :]
    out[256:320, 256:512] = wo[0, 64:128, :]


def partial_body(tokens, pre, post, wq, wk, wv, wg, wd, wo, pay):
    x = tokens[...].astype(f32)
    squares = jnp.sum(x * x, axis=1, keepdims=True)
    normed = (x * pre[0:1, :]).astype(bf16)
    hi = squares.astype(bf16).astype(f32)
    lane = lax.broadcasted_iota(jnp.int32, (256, 128), 1)
    for i, w in enumerate(columns(wq, wk, wv, wg, wd)):
        acc = jnp.dot(normed, w, preferred_element_type=f32)
        if i == 3:
            acc = jnp.where(lane == 64, hi, jnp.where(lane == 65, squares - hi, acc))
        pay[:, 0:LS, 128 * i : 128 * i + 128] = acc.astype(bf16).reshape(DP, LS, 128)
    pay[:, 0:LS, 512:768] = tokens[...].reshape(DP, LS, 256)
    row = lax.broadcasted_iota(jnp.int32, (8, 256), 0)
    gains = jnp.zeros((8, 256), f32)
    for i, g in enumerate((pre[1:2, :], post[0:1, :], post[1:2, :])):
        high = g.astype(bf16).astype(f32)
        gains = jnp.where(row == i, high, gains)
        gains = jnp.where(row == 3 + i, g - high, gains)
    gains = gains.astype(bf16)
    for half in range(2):
        start = 64 * half
        chunks = (
            wo[0, start : start + 24, :],
            wo[0, start + 24 : start + 48, :],
            jnp.concatenate([wo[0, start + 48 : start + 64, :], gains], axis=0),
        )
        for d in range(half, DP, 2):
            for i, chunk in enumerate(chunks):
                pay[d, LS:40, 256 * i : 256 * i + 256] = chunk


def attend(proj, squares, bias, gain, old, new_ref, wide, reads):
    scale = lax.rsqrt(squares / D + epsilon)
    lane = lax.broadcasted_iota(jnp.int32, (LS, 128), 1)
    low = lane < 64
    qk = (proj[:, 0:128] * scale).astype(bf16).astype(f32)
    kq = pltpu.roll(qk, 64, 1)
    query = jnp.where(low, qk, kq)
    key = jnp.where(low, kq, qk)
    value = proj[:, 128:256] * scale
    gate = proj[:, 256:384] * scale
    wide[0:1, 0:64] = bias
    wide[0:1, 64:128] = jnp.zeros((1, 64), f32)
    z = proj[:, 384:512] * scale + wide[0:1, :]
    log_decay = (jnp.minimum(z, 0.0) - jnp.log1p(jnp.exp(-jnp.abs(z)))) / 16.0
    decay = jnp.exp(log_decay)
    decay = jnp.where(low, decay, pltpu.roll(decay, 64, 1))
    right = (lane >= 64).astype(jnp.int32)
    for b in range(64):
        v = jnp.take_along_axis(value, right + 2 * b, axis=1)
        new = decay * old[0, :, b * 128 : b * 128 + 128] + key * v
        new_ref[0, :, b * 128 : b * 128 + 128] = new
        reads[b * LS : b * LS + LS, :] = query * new
    row = lax.broadcasted_iota(jnp.int32, (128, 128), 0)
    col = lax.broadcasted_iota(jnp.int32, (128, 128), 1)
    fold = ((row >= 64) == (col % 2 == 1)).astype(f32).astype(bf16)
    product = reads[...]
    high = product.astype(bf16)
    rest = (product - high.astype(f32)).astype(bf16)
    sums = jnp.dot(high, fold, preferred_element_type=f32) + jnp.dot(rest, fold, preferred_element_type=f32)
    readout = jnp.zeros((LS, 128), f32)
    for b in range(64):
        readout = jnp.where(lane // 2 == b, sums[b * LS : b * LS + LS, :], readout)
    readout = readout * KEY ** (-0.5)
    mean = jnp.sum(readout * readout, axis=1, keepdims=True) / VAL
    silu = gate / (1.0 + jnp.exp(-gate))
    return (readout * lax.rsqrt(mean + epsilon) * gain * silu).astype(bf16)


def first_state_body(got, bias, gain, old, new_ref, mixed, wide, reads):
    proj = got[0, 0:LS, 0:512].astype(f32)
    for d in range(1, DP):
        proj = proj + got[d, 0:LS, 0:512].astype(f32)
    squares = proj[:, 448:449] + proj[:, 449:450]
    mixed[...] = attend(proj, squares, bias[0:1, :], gain[0:1, :], old, new_ref, wide, reads)


def half_of(got, d):
    return [
        got[d, LS:40, 0:256],
        got[d, LS:40, 256:512],
        got[d, LS:32, 512:768],
    ]


def first_spread_body(mixed, got, swapped, out):
    m = mixed[...].astype(f32)
    m = jnp.where(lax.axis_index("dp") % 2 == 0, m, pltpu.roll(m, 64, 1)).astype(bf16)
    for d in range(DP):
        w = jnp.concatenate(half_of(got, d) + half_of(swapped, d), axis=0)
        part = jnp.dot(m, w, preferred_element_type=f32).astype(bf16)
        out[2 * d] = part[:, 0:128]
        out[2 * d + 1] = part[:, 128:256]


def second_body(normed, squares, bias, gain, old, kept, *refs):
    weights, outs = refs[:8], refs[8:16]
    new_ref, out, wide, reads = refs[16:]
    proj = jnp.zeros((LS, 512), f32)
    where = owners()
    for piece, pair in zip(weights, where):
        for j in range(2):
            proj = proj + jnp.dot(normed[pair[j]], piece[j], preferred_element_type=f32)
    m = attend(proj, squares[:, 0:1], bias[1:2, :], gain[1:2, :], old, new_ref, wide, reads)
    for piece, pair in zip(outs, where):
        for j in range(2):
            w = jnp.concatenate([piece[j, :, 0:256], piece[j, :, 256:512]], axis=0)
            part = jnp.dot(m, w, preferred_element_type=f32).astype(bf16)
            out[2 * pair[j]] = part[:, 0:128]
            out[2 * pair[j] + 1] = part[:, 128:256]


def total_body(arrived, out):
    total = arrived[0].astype(f32)
    for t in range(1, TP):
        total = total + arrived[t].astype(f32)
    total = total.astype(bf16)
    for t in range(TP):
        out[t] = total


def residual_body(b, full, x, gains, *outs):
    squares = jnp.zeros((LS, 128), f32)
    for t in range(TP):
        o = full[t].astype(f32)
        squares = squares + o * o
    scale = lax.rsqrt(jnp.sum(squares, axis=1, keepdims=True) / D + epsilon)
    after = jnp.zeros((LS, 256), f32)
    for d in range(DP):
        g = gains[d].astype(f32)
        o = jnp.concatenate([full[2 * d], full[2 * d + 1]], axis=1).astype(f32)
        post = g[1 + b : 2 + b, :] + g[4 + b : 5 + b, :]
        new = (x[d].astype(f32) + o * scale * post).astype(bf16)
        outs[0][d] = new
        if b == 0:
            wide = new.astype(f32)
            after = after + wide * wide
            outs[1][d] = (wide * (g[0:1, :] + g[3:4, :])).astype(bf16)
    if b == 0:
        total = jnp.sum(after, axis=1, keepdims=True)
        outs[2][...] = jnp.broadcast_to(total, (LS, 128))


def gathered(array, after):
    other = lax.ppermute(array, "dp", SWAP)
    own = jnp.stack([array, other])
    ring = []
    swapped = []
    now, after = lax.optimization_barrier((own, after))
    own = now
    for k in range(4):
        now = lax.ppermute(now, "dp", RING)
        ring.append(now)
        if k < 3:
            swapped.append(lax.ppermute(now, "dp", SWAP))
    return [own, *ring, *swapped], after


def shape(s, t=bf16):
    return jax.ShapeDtypeStruct(s, t)


def local(tokens, recurrent_state, pre_gain, w_query, w_key, w_value, w_gate, w_decay, decay_bias, head_gain, w_out, post_gain):
    turned = lambda w: jnp.swapaxes(w, 1, 2)
    weights = (turned(w_query), turned(w_key), w_value, w_gate, turned(w_decay))

    def weight_specs(b):
        return [whole((1, *w.shape[1:]), (b, 0, 0)) for w in weights]

    pay = call(
        partial_body,
        shape((DP, 40, 768)),
        [whole((256, 256)), whole((2, 256)), whole((2, 256)), *weight_specs(0), whole((1, 128, 256))],
        whole((DP, 40, 768)),
    )(tokens, pre_gain, post_gain, *weights, w_out)
    second = call(
        second_weights_body,
        shape((320, 512)),
        [*weight_specs(1), whole((1, 128, 256), (1, 0, 0))],
        whole((320, 512)),
    )(*weights, w_out)
    got = lax.all_to_all(pay, "dp", 0, 0, tiled=True)
    pieces1, got = gathered(second, got)
    swapped = lax.ppermute(got, "dp", SWAP)
    wide = [pltpu.VMEM((8, 128), f32), pltpu.VMEM((64 * LS, 128), f32)]
    state, mixed = call(
        first_state_body,
        [shape((2, LS, 8192), f32), shape((LS, 128))],
        [whole((DP, 40, 768)), whole((2, 64)), whole((2, 128)), whole((1, LS, 8192))],
        [whole((1, LS, 8192)), whole((LS, 128))],
        wide,
    )(got, decay_bias, head_gain, recurrent_state)
    spread = call(
        first_spread_body,
        shape((TP, LS, 128)),
        [whole((LS, 128))] + [whole((DP, 40, 768))] * 2,
        whole((TP, LS, 128)),
    )(mixed, got, swapped)
    x, x_spec = got, whole((DP, LS, 256), (0, 0, 2))
    for b in range(2):
        arrived = lax.all_to_all(spread, "tp", 0, 0, tiled=True)
        if b == 0:
            arrived, _ = lax.optimization_barrier((arrived, pieces1[2]))
        own = call(
            total_body, shape((TP, LS, 128)), [whole((TP, LS, 128))], whole((TP, LS, 128))
        )(arrived)
        full = lax.all_to_all(own, "tp", 0, 0, tiled=True)
        if b == 0:
            full, _ = lax.optimization_barrier((full, pieces1[3]))
        outs = [shape((DP, LS, 256))]
        if b == 0:
            outs += [shape((DP, LS, 256)), shape((LS, 128), f32)]
        results = call(
            functools.partial(residual_body, b),
            outs,
            [whole((TP, LS, 128)), x_spec, whole((DP, 8, 256), (0, 4, 2))],
            [whole(o.shape) for o in outs],
        )(full, x, got)
        x, x_spec = results[0], whole((DP, LS, 256))
        if b == 0:
            state, spread = call(
                second_body,
                [shape((2, LS, 8192), f32), shape((TP, LS, 128))],
                [whole((DP, LS, 256)), whole((LS, 128)), whole((2, 64)), whole((2, 128))]
                + [whole((1, LS, 8192), (1, 0, 0)), pl.BlockSpec(memory_space=pl.ANY)]
                + [whole((2, 256, 512))] * 8
                + [whole((2, 64, 512), (0, 4, 0))] * 8,
                [whole((1, LS, 8192), (1, 0, 0)), whole((TP, LS, 128))],
                wide,
                {5: 0},
            )(results[1], results[2], decay_bias, head_gain, recurrent_state, state, *pieces1, *pieces1)
    back = lax.all_to_all(x, "dp", 0, 0, tiled=True)
    return (back.reshape(256, 256), state)


def solution(mesh):
    in_specs = (
        P(None, "dp"),
        P(None, "dp", "tp"),
        P(None, "dp"),
        P(None, "dp", "tp"),
        P(None, "dp", "tp"),
        P(None, "dp", "tp"),
        P(None, "dp", "tp"),
        P(None, "dp", "tp"),
        P(None, "tp"),
        P(),
        P(None, "tp", "dp"),
        P(None, "dp"),
    )
    out_specs = (P(None, "dp"), P(None, "dp", "tp"))

    return jax.shard_map(local, mesh=mesh, in_specs=in_specs, out_specs=out_specs, check_vma=False)
```

```python
import jax
import jax.numpy as jnp
from jax import lax
from jax.experimental import pallas as pl
from jax.experimental.pallas import tpu as pltpu
from jax.sharding import PartitionSpec as P


D = 4096
KEY = 64
VAL = 128
DP = 16
TP = 32
LS = 16
epsilon = 1e-06
bf16 = jnp.bfloat16
f32 = jnp.float32

SWAP = [(d, d ^ 1) for d in range(DP)]
RING = [(2 * y, 2 * ((y + 1) % 8)) for y in range(8)] + [
    (2 * y + 1, 2 * ((y + 7) % 8) + 1) for y in range(8)
]


def whole(shape, index=None):
    at = index or (0,) * len(shape)
    return pl.BlockSpec(shape, lambda i, at=at: at)


def call(body, out_shape, in_specs, out_specs, scratch=(), aliases=None, limit=16):
    return pl.pallas_call(
        body,
        grid=(1,),
        out_shape=out_shape,
        in_specs=in_specs,
        out_specs=out_specs,
        scratch_shapes=scratch,
        input_output_aliases=aliases or {},
        compiler_params=pltpu.CompilerParams(vmem_limit_bytes=limit * 1024 * 1024),
    )


def owners():
    me = lax.axis_index("dp")
    y = me // 2
    c = me % 2
    sign = 2 * c - 1
    found = []
    for p in range(8):
        if p == 0:
            at, order = y, c
        elif p <= 4:
            at, order = (y + sign * p + 8) % 8, c
        else:
            at, order = (y - sign * (p - 4) + 8) % 8, 1 - c
        found.append((2 * at + order, 2 * at + 1 - order))
    return found


def columns(wq, wk, wv, wg, wd):
    qk = jnp.concatenate([wq[0], wk[0]], axis=0).astype(f32).T.astype(bf16)
    decay = jnp.concatenate([wd[0].astype(f32), jnp.zeros((64, 256), f32)], axis=0).T.astype(bf16)
    return (qk, wv[0], wg[0], decay)


def split3(value):
    high = value.astype(bf16).astype(f32)
    mid = (value - high).astype(bf16).astype(f32)
    return high, mid, value - high - mid


def place(acc, lane, start, values):
    for i, value in enumerate(values):
        acc = jnp.where(lane == start + i, value, acc)
    return acc


def partial_body(tokens, pre, wq, wk, wv, wg, wd, pay):
    x = tokens[...].astype(f32)
    squares = jnp.sum(x * x, axis=1, keepdims=True)
    normed = (x * pre[0:1, :]).astype(bf16)
    lane = lax.broadcasted_iota(jnp.int32, (256, 128), 1)
    for i, w in enumerate(columns(wq, wk, wv, wg, wd)):
        acc = jnp.dot(normed, w, preferred_element_type=f32)
        if i == 3:
            acc = place(acc, lane, 64, split3(squares))
        pay[:, :, 128 * i : 128 * i + 128] = acc.astype(bf16).reshape(DP, LS, 128)


def first_state_body(got, bias, gain, old, new_ref, mixed, wide, reads):
    proj = got[0].astype(f32)
    for d in range(1, DP):
        proj = proj + got[d].astype(f32)
    squares = proj[:, 448:449] + proj[:, 449:450] + proj[:, 450:451]
    m = attend(proj, squares, bias[0:1, :], gain[0:1, :], old, new_ref, wide, reads)
    for d in range(DP):
        mixed[d] = m


def first_out_body(mixed, wo, out):
    m = mixed[...].reshape(DP * LS, VAL)
    part = jnp.dot(m, wo[0], preferred_element_type=f32)
    out[...] = part.reshape(TP, 8, 256).astype(bf16)


def total_body(arrived, out):
    total = arrived[0].astype(f32)
    for t in range(1, TP):
        total = total + arrived[t].astype(f32)
    total = total.astype(bf16)
    for t in range(TP):
        out[t] = total


def second_partial_body(full, tokens, pre, post, wq, wk, wv, wg, wd, pay):
    x = tokens[...].astype(f32)
    out = full[...].astype(f32).reshape(256, 256)
    step = out * post[0:1, :]
    stats = []
    for value in (out * out, x * x, x * step, step * step):
        stats += split3(jnp.sum(value, axis=1, keepdims=True))
    gain = pre[1:2, :]
    lhs = ((step * gain).astype(bf16), (x * gain).astype(bf16))
    lane = lax.broadcasted_iota(jnp.int32, (256, 128), 1)
    for i, w in enumerate(columns(wq, wk, wv, wg, wd)):
        for j in range(2):
            acc = jnp.dot(lhs[j], w, preferred_element_type=f32)
            if i == 3 and j == 0:
                acc = place(acc, lane, 64, stats)
            at = 512 * j + 128 * i
            pay[:, :, at : at + 128] = acc.astype(bf16).reshape(DP, LS, 128)


def second_state_body(got, bias, gain, old, kept, *refs):
    pieces = refs[:8]
    new_ref, out, norm, wide, reads = refs[8:]
    total = got[0].astype(f32)
    for d in range(1, DP):
        total = total + got[d].astype(f32)
    stats = []
    for i in range(4):
        at = 448 + 3 * i
        stats.append(total[:, at : at + 1] + total[:, at + 1 : at + 2] + total[:, at + 2 : at + 3])
    scale = lax.rsqrt(stats[0] / D + epsilon)
    squares = stats[1] + 2.0 * scale * stats[2] + scale * scale * stats[3]
    proj = total[:, 512:1024] + scale * total[:, 0:512]
    norm[...] = jnp.broadcast_to(scale, (LS, 128))
    m = attend(proj, jnp.maximum(squares, 0.0), bias[1:2, :], gain[1:2, :], old, new_ref, wide, reads)
    for piece, pair in zip(pieces, owners()):
        for j in range(2):
            part = jnp.dot(m, piece[j], preferred_element_type=f32).astype(bf16)
            out[2 * pair[j]] = part[:, 0:128]
            out[2 * pair[j] + 1] = part[:, 128:256]


def scaled_body(full, norm, pay):
    squares = jnp.zeros((LS, 128), f32)
    for t in range(TP):
        o = full[t].astype(f32)
        squares = squares + o * o
    scale = lax.rsqrt(jnp.sum(squares, axis=1, keepdims=True) / D + epsilon)
    lane = lax.broadcasted_iota(jnp.int32, (LS, 128), 1)
    first = place(jnp.zeros((LS, 128), f32), lane, 0, split3(norm[...])).astype(bf16)
    for d in range(DP):
        pay[d, :, 0:128] = (full[2 * d].astype(f32) * scale).astype(bf16)
        pay[d, :, 128:256] = (full[2 * d + 1].astype(f32) * scale).astype(bf16)
        pay[d, :, 256:384] = first


def final_body(got, full, tokens, post, hidden):
    came = got[...].astype(f32).reshape(256, 384)
    scale = came[:, 256:257] + came[:, 257:258] + came[:, 258:259]
    out = full[...].astype(f32).reshape(256, 256)
    x = (tokens[...].astype(f32) + out * scale * post[0:1, :]).astype(bf16).astype(f32)
    hidden[...] = (x + came[:, 0:256] * post[1:2, :]).astype(bf16)


def attend(proj, squares, bias, gain, old, new_ref, wide, reads):
    scale = lax.rsqrt(squares / D + epsilon)
    lane = lax.broadcasted_iota(jnp.int32, (LS, 128), 1)
    low = lane < 64
    qk = (proj[:, 0:128] * scale).astype(bf16).astype(f32)
    kq = pltpu.roll(qk, 64, 1)
    query = jnp.where(low, qk, kq)
    key = jnp.where(low, kq, qk)
    value = proj[:, 128:256] * scale
    gate = proj[:, 256:384] * scale
    wide[0:1, 0:64] = bias
    wide[0:1, 64:128] = jnp.zeros((1, 64), f32)
    z = proj[:, 384:512] * scale + wide[0:1, :]
    log_decay = (jnp.minimum(z, 0.0) - jnp.log1p(jnp.exp(-jnp.abs(z)))) / 16.0
    decay = jnp.exp(log_decay)
    decay = jnp.where(low, decay, pltpu.roll(decay, 64, 1))
    right = (lane >= 64).astype(jnp.int32)
    for b in range(64):
        v = jnp.take_along_axis(value, right + 2 * b, axis=1)
        new = decay * old[0, :, b * 128 : b * 128 + 128] + key * v
        new_ref[0, :, b * 128 : b * 128 + 128] = new
        reads[b * LS : b * LS + LS, :] = query * new
    row = lax.broadcasted_iota(jnp.int32, (128, 128), 0)
    col = lax.broadcasted_iota(jnp.int32, (128, 128), 1)
    fold = ((row >= 64) == (col % 2 == 1)).astype(f32).astype(bf16)
    product = reads[...]
    high = product.astype(bf16)
    rest = (product - high.astype(f32)).astype(bf16)
    sums = jnp.dot(high, fold, preferred_element_type=f32) + jnp.dot(rest, fold, preferred_element_type=f32)
    readout = jnp.zeros((LS, 128), f32)
    for b in range(64):
        readout = jnp.where(lane // 2 == b, sums[b * LS : b * LS + LS, :], readout)
    readout = readout * KEY ** (-0.5)
    mean = jnp.sum(readout * readout, axis=1, keepdims=True) / VAL
    silu = gate / (1.0 + jnp.exp(-gate))
    return (readout * lax.rsqrt(mean + epsilon) * gain * silu).astype(bf16)


def gathered(array):
    other = lax.ppermute(array, "dp", SWAP)
    own = jnp.stack([array, other])
    ring = []
    swapped = []
    now = own
    for k in range(4):
        now = lax.ppermute(now, "dp", RING)
        ring.append(now)
        if k < 3:
            swapped.append(lax.ppermute(now, "dp", SWAP))
    return [own, *ring, *swapped]


def shape(s, t=bf16):
    return jax.ShapeDtypeStruct(s, t)


def local(tokens, recurrent_state, pre_gain, w_query, w_key, w_value, w_gate, w_decay, decay_bias, head_gain, w_out, post_gain):
    turned = lambda w: jnp.swapaxes(w, 1, 2)
    weights = (turned(w_query), turned(w_key), w_value, w_gate, turned(w_decay))

    def weight_specs(b):
        return [whole((1, *w.shape[1:]), (b, 0, 0)) for w in weights]

    def exchange(array, axis, beside=None):
        came = lax.all_to_all(array, axis, 0, 0, tiled=True)
        if beside is not None:
            came, _ = lax.optimization_barrier((came, beside))
        return came

    pair = whole((2, 256))
    pay = call(
        partial_body,
        shape((DP, LS, 512)),
        [whole((256, 256)), pair, *weight_specs(0)],
        whole((DP, LS, 512)),
        limit=60,
    )(tokens, pre_gain, *weights)
    pieces = gathered(w_out[1])
    got = exchange(pay, "dp", pieces[1])
    scratch = [pltpu.VMEM((8, 128), f32), pltpu.VMEM((64 * LS, 128), f32)]
    state, mixed = call(
        first_state_body,
        [shape((2, LS, 8192), f32), shape((DP, LS, 128))],
        [whole((DP, LS, 512)), whole((2, 64)), whole((2, 128)), whole((1, LS, 8192))],
        [whole((1, LS, 8192)), whole((DP, LS, 128))],
        scratch,
    )(got, decay_bias, head_gain, recurrent_state)
    mixed = exchange(mixed, "dp", pieces[2])
    spread = call(
        first_out_body,
        shape((TP, 8, 256)),
        [whole((DP, LS, 128)), whole((1, 128, 256))],
        whole((TP, 8, 256)),
    )(mixed, w_out)
    arrived = exchange(spread, "tp", pieces[3])
    own = call(total_body, shape((TP, 8, 256)), [whole((TP, 8, 256))], whole((TP, 8, 256)))(arrived)
    full0 = exchange(own, "tp", pieces[4])
    pay = call(
        second_partial_body,
        shape((DP, LS, 1024)),
        [whole((TP, 8, 256)), whole((256, 256)), pair, pair, *weight_specs(1)],
        whole((DP, LS, 1024)),
    )(full0, tokens, pre_gain, post_gain, *weights)
    got = exchange(pay, "dp")
    state, spread, norm = call(
        second_state_body,
        [shape((2, LS, 8192), f32), shape((TP, LS, 128)), shape((LS, 128), f32)],
        [whole((DP, LS, 1024)), whole((2, 64)), whole((2, 128))]
        + [whole((1, LS, 8192), (1, 0, 0)), pl.BlockSpec(memory_space=pl.ANY)]
        + [whole((2, 128, 256))] * 8,
        [whole((1, LS, 8192), (1, 0, 0)), whole((TP, LS, 128)), whole((LS, 128))],
        scratch,
        {4: 0},
    )(got, decay_bias, head_gain, recurrent_state, state, *pieces)
    arrived = exchange(spread, "tp")
    own = call(total_body, shape((TP, LS, 128)), [whole((TP, LS, 128))], whole((TP, LS, 128)))(arrived)
    full1 = exchange(own, "tp")
    pay = call(
        scaled_body,
        shape((DP, LS, 384)),
        [whole((TP, LS, 128)), whole((LS, 128))],
        whole((DP, LS, 384)),
    )(full1, norm)
    got = exchange(pay, "dp")
    hidden = call(
        final_body,
        shape((256, 256)),
        [whole((DP, LS, 384)), whole((TP, 8, 256)), whole((256, 256)), pair],
        whole((256, 256)),
    )(got, full0, tokens, post_gain)
    return (hidden, state)


def solution(mesh):
    in_specs = (
        P(None, "dp"),
        P(None, "dp", "tp"),
        P(None, "dp"),
        P(None, "dp", "tp"),
        P(None, "dp", "tp"),
        P(None, "dp", "tp"),
        P(None, "dp", "tp"),
        P(None, "dp", "tp"),
        P(None, "tp"),
        P(),
        P(None, "tp", "dp"),
        P(None, "dp"),
    )
    out_specs = (P(None, "dp"), P(None, "dp", "tp"))

    return jax.shard_map(local, mesh=mesh, in_specs=in_specs, out_specs=out_specs, check_vma=False)
```

```python
import jax
import jax.numpy as jnp
from jax import lax
from jax.experimental import pallas as pl
from jax.experimental.pallas import tpu as pltpu
from jax.sharding import PartitionSpec as P

D = 4096
KEY = 64
VAL = 128
DP = 16
TP = 32
LS = 16
epsilon = 1e-06
bf16 = jnp.bfloat16
f32 = jnp.float32

def whole(shape, index=None):
    at = index or (0,) * len(shape)
    return pl.BlockSpec(shape, lambda i, at=at: at)


def call(body, out_shape, in_specs, out_specs, scratch=(), aliases=None, limit=16):
    return pl.pallas_call(
        body,
        grid=(1,),
        out_shape=out_shape,
        in_specs=in_specs,
        out_specs=out_specs,
        scratch_shapes=scratch,
        input_output_aliases=aliases or {},
        compiler_params=pltpu.CompilerParams(vmem_limit_bytes=limit * 1024 * 1024),
    )


def columns(wq, wk, wv, wg, wd):
    qk = jnp.concatenate([wq[0], wk[0]], axis=0).astype(f32).T.astype(bf16)
    decay = jnp.concatenate([wd[0].astype(f32), jnp.zeros((64, 256), f32)], axis=0).T.astype(bf16)
    return (qk, wv[0], wg[0], decay)


def split3(value):
    high = value.astype(bf16).astype(f32)
    mid = (value - high).astype(bf16).astype(f32)
    return high, mid, value - high - mid


def place(acc, lane, start, values):
    for i, value in enumerate(values):
        acc = jnp.where(lane == start + i, value, acc)
    return acc


def partial_body(tokens, pre, wq, wk, wv, wg, wd, pay):
    x = tokens[...].astype(f32)
    squares = jnp.sum(x * x, axis=1, keepdims=True)
    normed = (x * pre[0:1, :]).astype(bf16)
    lane = lax.broadcasted_iota(jnp.int32, (256, 128), 1)
    for i, w in enumerate(columns(wq, wk, wv, wg, wd)):
        acc = jnp.dot(normed, w, preferred_element_type=f32)
        if i == 3:
            acc = place(acc, lane, 64, split3(squares))
        pay[:, :, 128 * i : 128 * i + 128] = acc.astype(bf16).reshape(DP, LS, 128)


def first_state_body(got, bias, gain, old, new_ref, mixed, wide, reads):
    proj = got[0].astype(f32)
    for d in range(1, DP):
        proj = proj + got[d].astype(f32)
    squares = proj[:, 448:449] + proj[:, 449:450] + proj[:, 450:451]
    m = attend(proj, squares, bias[0:1, :], gain[0:1, :], old, new_ref, wide, reads)
    for d in range(DP):
        mixed[d] = m


def first_out_body(mixed, wo, out):
    m = mixed[...].reshape(DP * LS, VAL)
    part = jnp.dot(m, wo[0], preferred_element_type=f32)
    out[...] = part.reshape(TP, 8, 256).astype(bf16)


def total_body(arrived, out):
    total = arrived[0].astype(f32)
    for t in range(1, TP):
        total = total + arrived[t].astype(f32)
    total = total.astype(bf16)
    for t in range(TP):
        out[t] = total


def second_partial_body(full, tokens, pre, post, wq, wk, wv, wg, wd, pay):
    x = tokens[...].astype(f32)
    out = full[...].astype(f32).reshape(256, 256)
    step = out * post[0:1, :]
    stats = []
    for value in (out * out, x * x, x * step, step * step):
        stats += split3(jnp.sum(value, axis=1, keepdims=True))
    gain = pre[1:2, :]
    lhs = ((step * gain).astype(bf16), (x * gain).astype(bf16))
    lane = lax.broadcasted_iota(jnp.int32, (256, 128), 1)
    for i, w in enumerate(columns(wq, wk, wv, wg, wd)):
        for j in range(2):
            acc = jnp.dot(lhs[j], w, preferred_element_type=f32)
            if i == 3 and j == 0:
                acc = place(acc, lane, 64, stats)
            at = 512 * j + 128 * i
            pay[:, :, at : at + 128] = acc.astype(bf16).reshape(DP, LS, 128)


def second_state_body(got, bias, gain, old, kept, new_ref, mixed, wide, reads):
    total = got[0].astype(f32)
    for d in range(1, DP):
        total = total + got[d].astype(f32)
    stats = []
    for i in range(4):
        at = 448 + 3 * i
        stats.append(total[:, at : at + 1] + total[:, at + 1 : at + 2] + total[:, at + 2 : at + 3])
    scale = lax.rsqrt(stats[0] / D + epsilon)
    squares = stats[1] + 2.0 * scale * stats[2] + scale * scale * stats[3]
    proj = total[:, 512:1024] + scale * total[:, 0:512]
    m = attend(proj, jnp.maximum(squares, 0.0), bias[1:2, :], gain[1:2, :], old, new_ref, wide, reads)
    for d in range(DP):
        mixed[d] = m


def squares_body(full1, full0, pay):
    lane = lax.broadcasted_iota(jnp.int32, (LS, 128), 1)
    acc = jnp.zeros((LS, 128), f32)
    for i, full in enumerate((full1, full0)):
        out = full[...].astype(f32).reshape(256, 256)
        parts = split3(jnp.sum(out * out, axis=1, keepdims=True))
        for d in range(DP):
            for j in range(3):
                acc = jnp.where(lane == 48 * i + 16 * j + d, parts[j][LS * d : LS * d + LS], acc)
    acc = acc.astype(bf16)
    for d in range(DP):
        pay[d] = acc


def final_body(got, full1, full0, tokens, post, hidden):
    total = got[0].astype(f32)
    for d in range(1, DP):
        total = total + got[d].astype(f32)
    total = total + pltpu.roll(total, 112, 1) + pltpu.roll(total, 96, 1)
    scale = lax.rsqrt(total / D + epsilon)
    for d in range(DP):
        at = slice(LS * d, LS * d + LS)
        outs = [full[2 * d : 2 * d + 2].astype(f32).reshape(LS, 256) for full in (full1, full0)]
        x = tokens[at, :].astype(f32) + outs[1] * scale[:, 48 + d : 49 + d] * post[0:1, :]
        x = x.astype(bf16).astype(f32)
        hidden[at, :] = (x + outs[0] * scale[:, d : d + 1] * post[1:2, :]).astype(bf16)


def attend(proj, squares, bias, gain, old, new_ref, wide, reads):
    scale = lax.rsqrt(squares / D + epsilon)
    lane = lax.broadcasted_iota(jnp.int32, (LS, 128), 1)
    low = lane < 64
    qk = (proj[:, 0:128] * scale).astype(bf16).astype(f32)
    kq = pltpu.roll(qk, 64, 1)
    query = jnp.where(low, qk, kq)
    key = jnp.where(low, kq, qk)
    value = proj[:, 128:256] * scale
    gate = proj[:, 256:384] * scale
    wide[0:1, 0:64] = bias
    wide[0:1, 64:128] = jnp.zeros((1, 64), f32)
    z = proj[:, 384:512] * scale + wide[0:1, :]
    log_decay = (jnp.minimum(z, 0.0) - jnp.log1p(jnp.exp(-jnp.abs(z)))) / 16.0
    decay = jnp.exp(log_decay)
    decay = jnp.where(low, decay, pltpu.roll(decay, 64, 1))
    right = (lane >= 64).astype(jnp.int32)
    for b in range(64):
        v = jnp.take_along_axis(value, right + 2 * b, axis=1)
        new = decay * old[0, :, b * 128 : b * 128 + 128] + key * v
        new_ref[0, :, b * 128 : b * 128 + 128] = new
        reads[b * LS : b * LS + LS, :] = query * new
    row = lax.broadcasted_iota(jnp.int32, (128, 128), 0)
    col = lax.broadcasted_iota(jnp.int32, (128, 128), 1)
    fold = ((row >= 64) == (col % 2 == 1)).astype(f32).astype(bf16)
    product = reads[...]
    high = product.astype(bf16)
    rest = (product - high.astype(f32)).astype(bf16)
    sums = jnp.dot(high, fold, preferred_element_type=f32) + jnp.dot(rest, fold, preferred_element_type=f32)
    readout = jnp.zeros((LS, 128), f32)
    for b in range(64):
        readout = jnp.where(lane // 2 == b, sums[b * LS : b * LS + LS, :], readout)
    readout = readout * KEY ** (-0.5)
    mean = jnp.sum(readout * readout, axis=1, keepdims=True) / VAL
    silu = gate / (1.0 + jnp.exp(-gate))
    return (readout * lax.rsqrt(mean + epsilon) * gain * silu).astype(bf16)


def shape(s, t=bf16):
    return jax.ShapeDtypeStruct(s, t)


def local(tokens, recurrent_state, pre_gain, w_query, w_key, w_value, w_gate, w_decay, decay_bias, head_gain, w_out, post_gain):
    turned = lambda w: jnp.swapaxes(w, 1, 2)
    weights = (turned(w_query), turned(w_key), w_value, w_gate, turned(w_decay))

    def weight_specs(b):
        return [whole((1, *w.shape[1:]), (b, 0, 0)) for w in weights]

    def exchange(array, axis):
        return lax.all_to_all(array, axis, 0, 0, tiled=True)

    pair = whole((2, 256))
    scratch = [pltpu.VMEM((8, 128), f32), pltpu.VMEM((64 * LS, 128), f32)]
    state_shapes = [shape((2, LS, 8192), f32), shape((DP, LS, 128))]
    out_spec = whole((TP, 8, 256))

    def shared(mixed, b):
        mixed = exchange(mixed, "dp")
        spread = call(
            first_out_body,
            shape((TP, 8, 256)),
            [whole((DP, LS, 128)), whole((1, 128, 256), (b, 0, 0))],
            out_spec,
        )(mixed, w_out)
        arrived = exchange(spread, "tp")
        own = call(total_body, shape((TP, 8, 256)), [out_spec], out_spec)(arrived)
        return exchange(own, "tp")

    pay = call(
        partial_body,
        shape((DP, LS, 512)),
        [whole((256, 256)), pair, *weight_specs(0)],
        whole((DP, LS, 512)),
        limit=60,
    )(tokens, pre_gain, *weights)
    got = exchange(pay, "dp")
    state, mixed = call(
        first_state_body,
        state_shapes,
        [whole((DP, LS, 512)), whole((2, 64)), whole((2, 128)), whole((1, LS, 8192))],
        [whole((1, LS, 8192)), whole((DP, LS, 128))],
        scratch,
    )(got, decay_bias, head_gain, recurrent_state)
    full0 = shared(mixed, 0)
    pay = call(
        second_partial_body,
        shape((DP, LS, 1024)),
        [out_spec, whole((256, 256)), pair, pair, *weight_specs(1)],
        whole((DP, LS, 1024)),
    )(full0, tokens, pre_gain, post_gain, *weights)
    got = exchange(pay, "dp")
    state, mixed = call(
        second_state_body,
        state_shapes,
        [whole((DP, LS, 1024)), whole((2, 64)), whole((2, 128))]
        + [whole((1, LS, 8192), (1, 0, 0)), pl.BlockSpec(memory_space=pl.ANY)],
        [whole((1, LS, 8192), (1, 0, 0)), whole((DP, LS, 128))],
        scratch,
        {4: 0},
    )(got, decay_bias, head_gain, recurrent_state, state)
    full1 = shared(mixed, 1)
    pay = call(
        squares_body,
        shape((DP, LS, 128)),
        [out_spec, out_spec],
        whole((DP, LS, 128)),
    )(full1, full0)
    got = exchange(pay, "dp")
    hidden = call(
        final_body,
        shape((256, 256)),
        [whole((DP, LS, 128)), out_spec, out_spec, whole((256, 256)), pair],
        whole((256, 256)),
    )(got, full1, full0, tokens, post_gain)
    return (hidden, state)


def solution(mesh):
    in_specs = (
        P(None, "dp"),
        P(None, "dp", "tp"),
        P(None, "dp"),
        P(None, "dp", "tp"),
        P(None, "dp", "tp"),
        P(None, "dp", "tp"),
        P(None, "dp", "tp"),
        P(None, "dp", "tp"),
        P(None, "tp"),
        P(),
        P(None, "tp", "dp"),
        P(None, "dp"),
    )
    out_specs = (P(None, "dp"), P(None, "dp", "tp"))

    return jax.shard_map(local, mesh=mesh, in_specs=in_specs, out_specs=out_specs, check_vma=False)
```

```python
import jax
import jax.numpy as jnp
from jax import lax
from jax.experimental import pallas as pl
from jax.experimental.pallas import tpu as pltpu
from jax.sharding import PartitionSpec as P

D = 4096
KEY = 64
VAL = 128
DP = 16
TP = 32
LS = 16
epsilon = 1e-06
bf16 = jnp.bfloat16
f32 = jnp.float32

def whole(shape, index=None):
    at = index or (0,) * len(shape)
    return pl.BlockSpec(shape, lambda i, at=at: at)


def call(body, out_shape, in_specs, out_specs, scratch=(), aliases=None, limit=16):
    return pl.pallas_call(
        body,
        grid=(1,),
        out_shape=out_shape,
        in_specs=in_specs,
        out_specs=out_specs,
        scratch_shapes=scratch,
        input_output_aliases=aliases or {},
        compiler_params=pltpu.CompilerParams(vmem_limit_bytes=limit * 1024 * 1024),
    )


def columns(wq, wk, wv, wg, wd):
    qk = jnp.concatenate([wq[0], wk[0]], axis=0).astype(f32).T.astype(bf16)
    decay = jnp.concatenate([wd[0].astype(f32), jnp.zeros((64, 256), f32)], axis=0).T.astype(bf16)
    return (qk, wv[0], wg[0], decay)


def split3(value):
    high = value.astype(bf16).astype(f32)
    mid = (value - high).astype(bf16).astype(f32)
    return high, mid, value - high - mid


def place(acc, lane, start, values):
    for i, value in enumerate(values):
        acc = jnp.where(lane == start + i, value, acc)
    return acc


def late_columns(wd):
    return jnp.concatenate([jnp.zeros((64, 256), f32), wd[0].astype(f32)], axis=0).T.astype(bf16)


def turned_columns(wq, wk):
    return jnp.concatenate([wq[0], wk[0]], axis=0).astype(f32).T.astype(bf16)


def partial_body(tokens, pre, wq, wk, wv, wg, wd, wd1, pay):
    x = tokens[...].astype(f32)
    squares = jnp.sum(x * x, axis=1, keepdims=True)
    normed = (x * pre[0:1, :]).astype(bf16)
    lane = lax.broadcasted_iota(jnp.int32, (256, 128), 1)
    for i, w in enumerate(columns(wq, wk, wv, wg, wd)):
        acc = jnp.dot(normed, w, preferred_element_type=f32)
        if i == 3:
            late = (x * pre[1:2, :]).astype(bf16)
            acc = acc + jnp.dot(late, late_columns(wd1), preferred_element_type=f32)
            acc = place(acc, lane, 125, split3(squares))
        pay[:, :, 128 * i : 128 * i + 128] = acc.astype(bf16).reshape(DP, LS, 128)


def summed(came, start):
    total = came[0, :, start : start + 128].astype(f32)
    for d in range(1, DP):
        total = total + came[d, :, start : start + 128].astype(f32)
    return total


def last_three(tile):
    return tile[:, 125:126] + tile[:, 126:127] + tile[:, 127:128]


def first_state_body(got, bias, gain, old, tokens, pre, wq1, wk1, new_ref, pay, wide, reads):
    tiles = [summed(got, 128 * i) for i in range(4)]
    m = attend(tiles, last_three(tiles[3]), bias[0:1, :], gain[0:1, :], old, new_ref, wide, reads)
    late = (tokens[...].astype(f32) * pre[1:2, :]).astype(bf16)
    part = jnp.dot(late, turned_columns(wq1, wk1), preferred_element_type=f32)
    pay[:, :, 128:256] = part.astype(bf16).reshape(DP, LS, 128)
    for d in range(DP):
        pay[d, :, 0:128] = m


def first_out_body(mixed, wo, out):
    m = mixed[...].reshape(DP * LS, VAL)
    part = jnp.dot(m, wo[0], preferred_element_type=f32)
    out[...] = part.reshape(TP, 8, 256).astype(bf16)


def total_body(arrived, out):
    total = arrived[0].astype(f32)
    for t in range(1, TP):
        total = total + arrived[t].astype(f32)
    total = total.astype(bf16)
    for t in range(TP):
        out[t] = total


def second_partial_body(full, tokens, pre, post, wq, wk, wv, wg, wd, pay):
    x = tokens[...].astype(f32)
    out = full[...].astype(f32).reshape(256, 256)
    step = out * post[0:1, :]
    stats = []
    for value in (out * out, x * step, step * step):
        stats += split3(jnp.sum(value, axis=1, keepdims=True))
    gain = pre[1:2, :]
    lhs, late = (step * gain).astype(bf16), (x * gain).astype(bf16)
    lane = lax.broadcasted_iota(jnp.int32, (256, 128), 1)
    tiles = columns(wq, wk, wv, wg, wd)
    results = [jnp.dot(lhs, w, preferred_element_type=f32) for w in tiles]
    ends = jnp.dot(late, late_columns(wd), preferred_element_type=f32)
    results[3] = place(jnp.where(lane >= 125, ends, results[3]), lane, 64, stats)
    results += [jnp.dot(late, w, preferred_element_type=f32) for w in tiles[1:3]]
    for i, acc in enumerate(results):
        pay[:, :, 128 * i : 128 * i + 128] = acc.astype(bf16).reshape(DP, LS, 128)


def second_state_body(got, first, mid, bias, gain, old, kept, new_ref, mixed, wide, reads):
    step = [summed(got, 128 * i) for i in range(4)]
    early = summed(first, 0)
    stats = []
    for i in range(3):
        at = 64 + 3 * i
        stats.append(step[3][:, at : at + 1] + step[3][:, at + 1 : at + 2] + step[3][:, at + 2 : at + 3])
    scale = lax.rsqrt(stats[0] / D + epsilon)
    squares = last_three(early) + 2.0 * scale * stats[1] + scale * scale * stats[2]
    lane = lax.broadcasted_iota(jnp.int32, (LS, 128), 1)
    decay = pltpu.roll(jnp.where(lane >= 125, step[3], early), 64, 1)
    base = [summed(mid, 0), summed(got, 512), summed(got, 640), decay]
    tiles = [x + scale * b for x, b in zip(base, step)]
    m = attend(tiles, jnp.maximum(squares, 0.0), bias[1:2, :], gain[1:2, :], old, new_ref, wide, reads)
    for d in range(DP):
        mixed[d] = m


def squares_body(full1, full0, pay):
    lane = lax.broadcasted_iota(jnp.int32, (LS, 128), 1)
    acc = jnp.zeros((LS, 128), f32)
    for i, full in enumerate((full1, full0)):
        out = full[...].astype(f32).reshape(256, 256)
        parts = split3(jnp.sum(out * out, axis=1, keepdims=True))
        for d in range(DP):
            for j in range(3):
                acc = jnp.where(lane == 48 * i + 16 * j + d, parts[j][LS * d : LS * d + LS], acc)
    acc = acc.astype(bf16)
    for d in range(DP):
        pay[d] = acc


def final_body(got, full1, full0, tokens, post, hidden):
    total = got[0].astype(f32)
    for d in range(1, DP):
        total = total + got[d].astype(f32)
    total = total + pltpu.roll(total, 112, 1) + pltpu.roll(total, 96, 1)
    scale = lax.rsqrt(total / D + epsilon)
    for d in range(DP):
        at = slice(LS * d, LS * d + LS)
        outs = [full[2 * d : 2 * d + 2].astype(f32).reshape(LS, 256) for full in (full1, full0)]
        x = tokens[at, :].astype(f32) + outs[1] * scale[:, 48 + d : 49 + d] * post[0:1, :]
        x = x.astype(bf16).astype(f32)
        hidden[at, :] = (x + outs[0] * scale[:, d : d + 1] * post[1:2, :]).astype(bf16)


def attend(tiles, squares, bias, gain, old, new_ref, wide, reads):
    scale = lax.rsqrt(squares / D + epsilon)
    lane = lax.broadcasted_iota(jnp.int32, (LS, 128), 1)
    low = lane < 64
    qk = (tiles[0] * scale).astype(bf16).astype(f32)
    kq = pltpu.roll(qk, 64, 1)
    query = jnp.where(low, qk, kq)
    key = jnp.where(low, kq, qk)
    value = tiles[1] * scale
    gate = tiles[2] * scale
    wide[0:1, 0:64] = bias
    wide[0:1, 64:128] = jnp.zeros((1, 64), f32)
    z = tiles[3] * scale + wide[0:1, :]
    log_decay = (jnp.minimum(z, 0.0) - jnp.log1p(jnp.exp(-jnp.abs(z)))) / 16.0
    decay = jnp.exp(log_decay)
    decay = jnp.where(low, decay, pltpu.roll(decay, 64, 1))
    right = (lane >= 64).astype(jnp.int32)
    for b in range(64):
        v = jnp.take_along_axis(value, right + 2 * b, axis=1)
        new = decay * old[0, :, b * 128 : b * 128 + 128] + key * v
        new_ref[0, :, b * 128 : b * 128 + 128] = new
        reads[b * LS : b * LS + LS, :] = query * new
    row = lax.broadcasted_iota(jnp.int32, (128, 128), 0)
    col = lax.broadcasted_iota(jnp.int32, (128, 128), 1)
    fold = ((row >= 64) == (col % 2 == 1)).astype(f32).astype(bf16)
    product = reads[...]
    high = product.astype(bf16)
    rest = (product - high.astype(f32)).astype(bf16)
    sums = jnp.dot(high, fold, preferred_element_type=f32) + jnp.dot(rest, fold, preferred_element_type=f32)
    readout = jnp.zeros((LS, 128), f32)
    for b in range(64):
        readout = jnp.where(lane // 2 == b, sums[b * LS : b * LS + LS, :], readout)
    readout = readout * KEY ** (-0.5)
    mean = jnp.sum(readout * readout, axis=1, keepdims=True) / VAL
    silu = gate / (1.0 + jnp.exp(-gate))
    return (readout * lax.rsqrt(mean + epsilon) * gain * silu).astype(bf16)


def shape(s, t=bf16):
    return jax.ShapeDtypeStruct(s, t)


def local(tokens, recurrent_state, pre_gain, w_query, w_key, w_value, w_gate, w_decay, decay_bias, head_gain, w_out, post_gain):
    turned = lambda w: jnp.swapaxes(w, 1, 2)
    weights = (turned(w_query), turned(w_key), w_value, w_gate, turned(w_decay))

    def weight_specs(b):
        return [whole((1, *w.shape[1:]), (b, 0, 0)) for w in weights]

    def exchange(array, axis):
        return lax.all_to_all(array, axis, 0, 0, tiled=True)

    pair = whole((2, 256))
    second_narrow = whole((1, 64, 256), (1, 0, 0))
    scratch = [pltpu.VMEM((8, 128), f32), pltpu.VMEM((64 * LS, 128), f32)]
    out_spec = whole((TP, 8, 256))

    def shared(mixed, b):
        spread = call(
            first_out_body,
            shape((TP, 8, 256)),
            [whole((DP, LS, 128)), whole((1, 128, 256), (b, 0, 0))],
            out_spec,
        )(mixed, w_out)
        arrived = exchange(spread, "tp")
        own = call(total_body, shape((TP, 8, 256)), [out_spec], out_spec)(arrived)
        return exchange(own, "tp")

    pay = call(
        partial_body,
        shape((DP, LS, 512)),
        [whole((256, 256)), pair, *weight_specs(0), second_narrow],
        whole((DP, LS, 512)),
    )(*(pltpu.with_memory_space_constraint(a, pltpu.HBM) for a in (tokens, pre_gain, *weights, weights[4])))
    got = exchange(pay, "dp")
    state, mixed = call(
        first_state_body,
        [shape((2, LS, 8192), f32), shape((DP, LS, 256))],
        [whole((DP, LS, 512)), whole((2, 64)), whole((2, 128)), whole((1, LS, 8192))]
        + [whole((256, 256)), pair, second_narrow, second_narrow],
        [whole((1, LS, 8192)), whole((DP, LS, 256))],
        scratch,
    )(got, decay_bias, head_gain, recurrent_state, tokens, pre_gain, weights[0], weights[1])
    first, mid = got, exchange(mixed, "dp")
    full0 = shared(mid, 0)
    pay = call(
        second_partial_body,
        shape((DP, LS, 768)),
        [out_spec, whole((256, 256)), pair, pair, *weight_specs(1)],
        whole((DP, LS, 768)),
    )(full0, tokens, pre_gain, post_gain, *weights)
    got = exchange(pay, "dp")
    state, mixed = call(
        second_state_body,
        [shape((2, LS, 8192), f32), shape((DP, LS, 128))],
        [whole((DP, LS, 768)), whole((DP, LS, 128), (0, 0, 3)), whole((DP, LS, 128), (0, 0, 1))]
        + [whole((2, 64)), whole((2, 128))]
        + [whole((1, LS, 8192), (1, 0, 0)), pl.BlockSpec(memory_space=pl.ANY)],
        [whole((1, LS, 8192), (1, 0, 0)), whole((DP, LS, 128))],
        scratch,
        {6: 0},
    )(got, first, mid, decay_bias, head_gain, recurrent_state, state)
    full1 = shared(exchange(mixed, "dp"), 1)
    pay = call(
        squares_body,
        shape((DP, LS, 128)),
        [out_spec, out_spec],
        whole((DP, LS, 128)),
    )(full1, full0)
    got = exchange(pay, "dp")
    hidden = call(
        final_body,
        shape((256, 256)),
        [whole((DP, LS, 128)), out_spec, out_spec, whole((256, 256)), pair],
        whole((256, 256)),
    )(got, full1, full0, tokens, post_gain)
    return (hidden, state)


def solution(mesh):
    in_specs = (
        P(None, "dp"),
        P(None, "dp", "tp"),
        P(None, "dp"),
        P(None, "dp", "tp"),
        P(None, "dp", "tp"),
        P(None, "dp", "tp"),
        P(None, "dp", "tp"),
        P(None, "dp", "tp"),
        P(None, "tp"),
        P(),
        P(None, "tp", "dp"),
        P(None, "dp"),
    )
    out_specs = (P(None, "dp"), P(None, "dp", "tp"))

    return jax.shard_map(local, mesh=mesh, in_specs=in_specs, out_specs=out_specs, check_vma=False)
```

```python
import jax
import jax.numpy as jnp
from jax import lax
from jax.experimental import pallas as pl
from jax.experimental.pallas import tpu as pltpu
from jax.sharding import PartitionSpec as P

D = 4096
KEY = 64
VAL = 128
DP = 16
TP = 32
LS = 16
epsilon = 1e-06
bf16 = jnp.bfloat16
f32 = jnp.float32

def whole(shape, index=None):
    at = index or (0,) * len(shape)
    return pl.BlockSpec(shape, lambda i, at=at: at)


def call(body, out_shape, in_specs, out_specs, scratch=(), aliases=None, limit=16):
    return pl.pallas_call(
        body,
        grid=(1,),
        out_shape=out_shape,
        in_specs=in_specs,
        out_specs=out_specs,
        scratch_shapes=scratch,
        input_output_aliases=aliases or {},
        compiler_params=pltpu.CompilerParams(vmem_limit_bytes=limit * 1024 * 1024),
    )


def columns(wq, wk, wv, wg, wd):
    qk = jnp.concatenate([wq[0], wk[0]], axis=0).astype(f32).T.astype(bf16)
    decay = jnp.concatenate([wd[0].astype(f32), jnp.zeros((64, 256), f32)], axis=0).T.astype(bf16)
    return (qk, wv[0], wg[0], decay)


def split3(value):
    high = value.astype(bf16).astype(f32)
    mid = (value - high).astype(bf16).astype(f32)
    return high, mid, value - high - mid


def place(acc, lane, start, values):
    for i, value in enumerate(values):
        acc = jnp.where(lane == start + i, value, acc)
    return acc


def late_columns(wd):
    return jnp.concatenate([jnp.zeros((64, 256), f32), wd[0].astype(f32)], axis=0).T.astype(bf16)


def partial_body(tokens, pre, wq, wk, wv, wg, wd, wd1, pay):
    x = tokens[...].astype(f32)
    squares = jnp.sum(x * x, axis=1, keepdims=True)
    normed = (x * pre[0:1, :]).astype(bf16)
    lane = lax.broadcasted_iota(jnp.int32, (256, 128), 1)
    for i, w in enumerate(columns(wq, wk, wv, wg, wd)):
        acc = jnp.dot(normed, w, preferred_element_type=f32)
        if i == 3:
            late = (x * pre[1:2, :]).astype(bf16)
            acc = acc + jnp.dot(late, late_columns(wd1), preferred_element_type=f32)
            acc = place(acc, lane, 125, split3(squares))
        pay[:, :, 128 * i : 128 * i + 128] = acc.astype(bf16).reshape(DP, LS, 128)


def summed(came, start):
    total = came[0, :, start : start + 128].astype(f32)
    for d in range(1, DP):
        total = total + came[d, :, start : start + 128].astype(f32)
    return total


def last_three(tile):
    return tile[:, 125:126] + tile[:, 126:127] + tile[:, 127:128]


def first_state_body(got, bias, gain, old, new_ref, mixed, wide, reads):
    tiles = [summed(got, 128 * i) for i in range(4)]
    m = attend(tiles, last_three(tiles[3]), bias[0:1, :], gain[0:1, :], old, new_ref, wide, reads)
    for d in range(DP):
        mixed[d] = m


def first_out_body(mixed, wo, out):
    m = mixed[...].reshape(DP * LS, VAL)
    part = jnp.dot(m, wo[0], preferred_element_type=f32)
    out[...] = part.reshape(TP, 8, 256).astype(bf16)


def total_body(arrived, out):
    total = arrived[0].astype(f32)
    for t in range(1, TP):
        total = total + arrived[t].astype(f32)
    total = total.astype(bf16)
    for t in range(TP):
        out[t] = total


def second_partial_body(full, tokens, pre, post, wq, wk, wv, wg, wd, pay):
    x = tokens[...].astype(f32)
    out = full[...].astype(f32).reshape(256, 256)
    step = out * post[0:1, :]
    stats = []
    for value in (out * out, x * step, step * step):
        stats += split3(jnp.sum(value, axis=1, keepdims=True))
    gain = pre[1:2, :]
    lhs, late = (step * gain).astype(bf16), (x * gain).astype(bf16)
    lane = lax.broadcasted_iota(jnp.int32, (256, 128), 1)
    tiles = columns(wq, wk, wv, wg, wd)
    results = [jnp.dot(lhs, w, preferred_element_type=f32) for w in tiles]
    ends = jnp.dot(late, late_columns(wd), preferred_element_type=f32)
    results[3] = place(jnp.where(lane >= 125, ends, results[3]), lane, 64, stats)
    results += [jnp.dot(late, w, preferred_element_type=f32) for w in tiles[0:3]]
    for i, acc in enumerate(results):
        pay[:, :, 128 * i : 128 * i + 128] = acc.astype(bf16).reshape(DP, LS, 128)


def second_state_body(got, first, bias, gain, old, kept, new_ref, mixed, wide, reads):
    step = [summed(got, 128 * i) for i in range(4)]
    early = summed(first, 0)
    stats = []
    for i in range(3):
        at = 64 + 3 * i
        stats.append(step[3][:, at : at + 1] + step[3][:, at + 1 : at + 2] + step[3][:, at + 2 : at + 3])
    scale = lax.rsqrt(stats[0] / D + epsilon)
    squares = last_three(early) + 2.0 * scale * stats[1] + scale * scale * stats[2]
    lane = lax.broadcasted_iota(jnp.int32, (LS, 128), 1)
    decay = pltpu.roll(jnp.where(lane >= 125, step[3], early), 64, 1)
    base = [summed(got, 512), summed(got, 640), summed(got, 768), decay]
    tiles = [x + scale * b for x, b in zip(base, step)]
    m = attend(tiles, jnp.maximum(squares, 0.0), bias[1:2, :], gain[1:2, :], old, new_ref, wide, reads)
    for d in range(DP):
        mixed[d] = m


def squares_body(full1, full0, pay):
    lane = lax.broadcasted_iota(jnp.int32, (8, 128), 1)
    acc = jnp.zeros((8, 128), f32)
    for i, full in enumerate((full1, full0)):
        out = full[...].astype(f32).reshape(256, 256)
        total = jnp.sum(out * out, axis=1, keepdims=True)
        high = total.astype(bf16).astype(f32)
        for j, part in enumerate((high, total - high)):
            for t in range(TP):
                acc = jnp.where(lane == 64 * i + 32 * j + t, part[8 * t : 8 * t + 8], acc)
    acc = acc.astype(bf16)
    for d in range(DP):
        pay[d] = acc


def final_body(got, full1, full0, tokens, post, hidden):
    total = got[0].astype(f32)
    for d in range(1, DP):
        total = total + got[d].astype(f32)
    scale = lax.rsqrt((total + pltpu.roll(total, 96, 1)) / D + epsilon)
    for d in range(DP):
        at = slice(LS * d, LS * d + LS)
        outs = [full[2 * d : 2 * d + 2].astype(f32).reshape(LS, 256) for full in (full1, full0)]
        rates = [
            jnp.concatenate([scale[:, i : i + 1], scale[:, i + 1 : i + 2]], axis=0)
            for i in (2 * d, 64 + 2 * d)
        ]
        x = tokens[at, :].astype(f32) + outs[1] * rates[1] * post[0:1, :]
        x = x.astype(bf16).astype(f32)
        hidden[at, :] = (x + outs[0] * rates[0] * post[1:2, :]).astype(bf16)


def attend(tiles, squares, bias, gain, old, new_ref, wide, reads):
    scale = lax.rsqrt(squares / D + epsilon)
    lane = lax.broadcasted_iota(jnp.int32, (LS, 128), 1)
    low = lane < 64
    qk = (tiles[0] * scale).astype(bf16).astype(f32)
    kq = pltpu.roll(qk, 64, 1)
    query = jnp.where(low, qk, kq)
    key = jnp.where(low, kq, qk)
    value = tiles[1] * scale
    gate = tiles[2] * scale
    wide[0:1, 0:64] = bias
    wide[0:1, 64:128] = jnp.zeros((1, 64), f32)
    z = tiles[3] * scale + wide[0:1, :]
    log_decay = (jnp.minimum(z, 0.0) - jnp.log1p(jnp.exp(-jnp.abs(z)))) / 16.0
    decay = jnp.exp(log_decay)
    decay = jnp.where(low, decay, pltpu.roll(decay, 64, 1))
    right = (lane >= 64).astype(jnp.int32)
    for b in range(64):
        v = jnp.take_along_axis(value, right + 2 * b, axis=1)
        new = decay * old[0, :, b * 128 : b * 128 + 128] + key * v
        new_ref[0, :, b * 128 : b * 128 + 128] = new
        reads[b * LS : b * LS + LS, :] = (query * new).astype(bf16)
    row = lax.broadcasted_iota(jnp.int32, (128, 128), 0)
    col = lax.broadcasted_iota(jnp.int32, (128, 128), 1)
    fold = ((row >= 64) == (col % 2 == 1)).astype(f32).astype(bf16)
    sums = jnp.dot(reads[...], fold, preferred_element_type=f32)
    readout = jnp.zeros((LS, 128), f32)
    for b in range(64):
        readout = jnp.where(lane // 2 == b, sums[b * LS : b * LS + LS, :], readout)
    readout = readout * KEY ** (-0.5)
    mean = jnp.sum(readout * readout, axis=1, keepdims=True) / VAL
    silu = gate / (1.0 + jnp.exp(-gate))
    return (readout * lax.rsqrt(mean + epsilon) * gain * silu).astype(bf16)


def shape(s, t=bf16):
    return jax.ShapeDtypeStruct(s, t)


def local(tokens, recurrent_state, pre_gain, w_query, w_key, w_value, w_gate, w_decay, decay_bias, head_gain, w_out, post_gain):
    turned = lambda w: jnp.swapaxes(w, 1, 2)
    weights = (turned(w_query), turned(w_key), w_value, w_gate, turned(w_decay))

    def weight_specs(b):
        return [whole((1, *w.shape[1:]), (b, 0, 0)) for w in weights]

    def exchange(array, axis):
        return lax.all_to_all(array, axis, 0, 0, tiled=True)

    pair = whole((2, 256))
    second_narrow = whole((1, 64, 256), (1, 0, 0))
    scratch = [pltpu.VMEM((8, 128), f32), pltpu.VMEM((64 * LS, 128), bf16)]
    out_spec = whole((TP, 8, 256))

    def shared(mixed, b):
        spread = call(
            first_out_body,
            shape((TP, 8, 256)),
            [whole((DP, LS, 128)), whole((1, 128, 256), (b, 0, 0))],
            out_spec,
        )(mixed, w_out)
        arrived = exchange(spread, "tp")
        own = call(total_body, shape((TP, 8, 256)), [out_spec], out_spec)(arrived)
        return exchange(own, "tp")

    pay = call(
        partial_body,
        shape((DP, LS, 512)),
        [whole((256, 256)), pair, *weight_specs(0), second_narrow],
        whole((DP, LS, 512)),
    )(*(pltpu.with_memory_space_constraint(a, pltpu.HBM) for a in (tokens, pre_gain, *weights, weights[4])))
    got = exchange(pay, "dp")
    state, mixed = call(
        first_state_body,
        [shape((2, LS, 8192), f32), shape((DP, LS, 128))],
        [whole((DP, LS, 512)), whole((2, 64)), whole((2, 128)), whole((1, LS, 8192))],
        [whole((1, LS, 8192)), whole((DP, LS, 128))],
        scratch,
    )(got, decay_bias, head_gain, recurrent_state)
    first = got
    full0 = shared(exchange(mixed, "dp"), 0)
    pay = call(
        second_partial_body,
        shape((DP, LS, 896)),
        [out_spec, whole((256, 256)), pair, pair, *weight_specs(1)],
        whole((DP, LS, 896)),
    )(full0, tokens, pre_gain, post_gain, *weights)
    got = exchange(pay, "dp")
    state, mixed = call(
        second_state_body,
        [shape((2, LS, 8192), f32), shape((DP, LS, 128))],
        [whole((DP, LS, 896)), whole((DP, LS, 128), (0, 0, 3))]
        + [whole((2, 64)), whole((2, 128))]
        + [whole((1, LS, 8192), (1, 0, 0)), pl.BlockSpec(memory_space=pl.ANY)],
        [whole((1, LS, 8192), (1, 0, 0)), whole((DP, LS, 128))],
        scratch,
        {5: 0},
    )(got, first, decay_bias, head_gain, recurrent_state, state)
    full1 = shared(exchange(mixed, "dp"), 1)
    pay = call(
        squares_body,
        shape((DP, 8, 128)),
        [out_spec, out_spec],
        whole((DP, 8, 128)),
    )(full1, full0)
    got = exchange(pay, "dp")
    hidden = call(
        final_body,
        shape((256, 256)),
        [whole((DP, 8, 128)), out_spec, out_spec, whole((256, 256)), pair],
        whole((256, 256)),
    )(got, full1, full0, tokens, post_gain)
    return (hidden, state)


def solution(mesh):
    in_specs = (
        P(None, "dp"),
        P(None, "dp", "tp"),
        P(None, "dp"),
        P(None, "dp", "tp"),
        P(None, "dp", "tp"),
        P(None, "dp", "tp"),
        P(None, "dp", "tp"),
        P(None, "dp", "tp"),
        P(None, "tp"),
        P(),
        P(None, "tp", "dp"),
        P(None, "dp"),
    )
    out_specs = (P(None, "dp"), P(None, "dp", "tp"))

    return jax.shard_map(local, mesh=mesh, in_specs=in_specs, out_specs=out_specs, check_vma=False)
```

```python
import jax
import jax.numpy as jnp
from jax import lax
from jax.experimental import pallas as pl
from jax.experimental.pallas import tpu as pltpu
from jax.sharding import PartitionSpec as P

D = 4096
KEY = 64
VAL = 128
DP = 16
TP = 32
LS = 16
epsilon = 1e-06
bf16 = jnp.bfloat16
f32 = jnp.float32

def whole(shape, index=None):
    at = index or (0,) * len(shape)
    return pl.BlockSpec(shape, lambda i, at=at: at)


def call(body, out_shape, in_specs, out_specs, scratch=(), aliases=None, limit=16):
    return pl.pallas_call(
        body,
        grid=(1,),
        out_shape=out_shape,
        in_specs=in_specs,
        out_specs=out_specs,
        scratch_shapes=scratch,
        input_output_aliases=aliases or {},
        compiler_params=pltpu.CompilerParams(vmem_limit_bytes=limit * 1024 * 1024),
    )


def columns(wq, wk, wv, wg, wd):
    qk = jnp.concatenate([wq[0], wk[0]], axis=0).astype(f32).T.astype(bf16)
    decay = jnp.concatenate([wd[0].astype(f32), jnp.zeros((64, 256), f32)], axis=0).T.astype(bf16)
    return (qk, wv[0], wg[0], decay)


def split3(value):
    high = value.astype(bf16).astype(f32)
    mid = (value - high).astype(bf16).astype(f32)
    return high, mid, value - high - mid


def place(acc, lane, start, values):
    for i, value in enumerate(values):
        acc = jnp.where(lane == start + i, value, acc)
    return acc


def late_columns(wd):
    return jnp.concatenate([jnp.zeros((64, 256), f32), wd[0].astype(f32)], axis=0).T.astype(bf16)


def turned_columns(wq, wk):
    return jnp.concatenate([wq[0], wk[0]], axis=0).astype(f32).T.astype(bf16)


def partial_body(tokens, pre, wq, wk, wv, wg, wd, wd1, pay):
    x = tokens[...].astype(f32)
    squares = jnp.sum(x * x, axis=1, keepdims=True)
    normed = (x * pre[0:1, :]).astype(bf16)
    lane = lax.broadcasted_iota(jnp.int32, (256, 128), 1)
    for i, w in enumerate(columns(wq, wk, wv, wg, wd)):
        acc = jnp.dot(normed, w, preferred_element_type=f32)
        if i == 3:
            late = (x * pre[1:2, :]).astype(bf16)
            acc = acc + jnp.dot(late, late_columns(wd1), preferred_element_type=f32)
            acc = place(acc, lane, 125, split3(squares))
        pay[:, :, 128 * i : 128 * i + 128] = acc.astype(bf16).reshape(DP, LS, 128)


def summed(came, start):
    total = came[0, :, start : start + 128].astype(f32)
    for d in range(1, DP):
        total = total + came[d, :, start : start + 128].astype(f32)
    return total


def last_three(tile):
    return tile[:, 125:126] + tile[:, 126:127] + tile[:, 127:128]


def first_state_body(got, bias, gain, old, tokens, pre, wq1, wk1, new_ref, pay, wide, reads):
    tiles = [summed(got, 128 * i) for i in range(4)]
    m = attend(tiles, last_three(tiles[3]), bias[0:1, :], gain[0:1, :], old, new_ref, wide, reads)
    late = (tokens[...].astype(f32) * pre[1:2, :]).astype(bf16)
    part = jnp.dot(late, turned_columns(wq1, wk1), preferred_element_type=f32)
    pay[:, :, 128:256] = part.astype(bf16).reshape(DP, LS, 128)
    for d in range(DP):
        pay[d, :, 0:128] = m


def first_out_body(mixed, wo, out):
    m = mixed[...].reshape(DP * LS, VAL)
    part = jnp.dot(m, wo[0], preferred_element_type=f32)
    out[...] = part.reshape(TP, 8, 256).astype(bf16)


def total_body(arrived, out):
    total = arrived[0].astype(f32)
    for t in range(1, TP):
        total = total + arrived[t].astype(f32)
    total = total.astype(bf16)
    for t in range(TP):
        out[t] = total


def second_partial_body(full, tokens, pre, post, wq, wk, wv, wg, wd, pay):
    x = tokens[...].astype(f32)
    out = full[...].astype(f32).reshape(256, 256)
    step = out * post[0:1, :]
    stats = []
    for value in (out * out, x * step, step * step):
        stats += split3(jnp.sum(value, axis=1, keepdims=True))
    gain = pre[1:2, :]
    lhs, late = (step * gain).astype(bf16), (x * gain).astype(bf16)
    lane = lax.broadcasted_iota(jnp.int32, (256, 128), 1)
    tiles = columns(wq, wk, wv, wg, wd)
    results = [jnp.dot(lhs, w, preferred_element_type=f32) for w in tiles]
    ends = jnp.dot(late, late_columns(wd), preferred_element_type=f32)
    results[3] = place(jnp.where(lane >= 125, ends, results[3]), lane, 64, stats)
    results += [jnp.dot(late, w, preferred_element_type=f32) for w in tiles[1:3]]
    for i, acc in enumerate(results):
        pay[:, :, 128 * i : 128 * i + 128] = acc.astype(bf16).reshape(DP, LS, 128)


def second_state_body(got, first, mid, bias, gain, old, kept, new_ref, mixed, wide, reads):
    step = [summed(got, 128 * i) for i in range(4)]
    early = summed(first, 0)
    stats = []
    for i in range(3):
        at = 64 + 3 * i
        stats.append(step[3][:, at : at + 1] + step[3][:, at + 1 : at + 2] + step[3][:, at + 2 : at + 3])
    scale = lax.rsqrt(stats[0] / D + epsilon)
    squares = last_three(early) + 2.0 * scale * stats[1] + scale * scale * stats[2]
    lane = lax.broadcasted_iota(jnp.int32, (LS, 128), 1)
    decay = pltpu.roll(jnp.where(lane >= 125, step[3], early), 64, 1)
    base = [summed(mid, 0), summed(got, 512), summed(got, 640), decay]
    tiles = [x + scale * b for x, b in zip(base, step)]
    m = attend(tiles, jnp.maximum(squares, 0.0), bias[1:2, :], gain[1:2, :], old, new_ref, wide, reads)
    for d in range(DP):
        mixed[d] = m


def squares_body(arrived, own0, total, pay):
    out = arrived[0].astype(f32)
    for t in range(1, TP):
        out = out + arrived[t].astype(f32)
    total[...] = out
    before = own0[0].astype(f32)
    lane = lax.broadcasted_iota(jnp.int32, (8, 128), 1)
    parts = []
    for value in (out, before):
        parts += split3(jnp.sum(value * value, axis=1, keepdims=True))
    acc = place(jnp.zeros((8, 128), f32), lane, 0, parts).astype(bf16)
    for d in range(DP):
        pay[d] = acc


def final_body(got, total, own0, tokens, post, out):
    came = got[0].astype(f32)
    for d in range(1, DP):
        came = came + got[d].astype(f32)
    rates = []
    for i in range(2):
        squares = came[:, 3 * i : 3 * i + 1] + came[:, 3 * i + 1 : 3 * i + 2] + came[:, 3 * i + 2 : 3 * i + 3]
        rates.append(lax.rsqrt(squares / D + epsilon))
    x = tokens[lax.axis_index("tp")].astype(f32)
    x = (x + own0[0].astype(f32) * rates[1] * post[0:1, :]).astype(bf16).astype(f32)
    x = (x + total[...] * rates[0] * post[1:2, :]).astype(bf16)
    for t in range(TP):
        out[t] = x


def attend(tiles, squares, bias, gain, old, new_ref, wide, reads):
    scale = lax.rsqrt(squares / D + epsilon)
    lane = lax.broadcasted_iota(jnp.int32, (LS, 128), 1)
    low = lane < 64
    qk = (tiles[0] * scale).astype(bf16).astype(f32)
    kq = pltpu.roll(qk, 64, 1)
    query = jnp.where(low, qk, kq)
    key = jnp.where(low, kq, qk)
    value = tiles[1] * scale
    gate = tiles[2] * scale
    wide[0:1, 0:64] = bias
    wide[0:1, 64:128] = jnp.zeros((1, 64), f32)
    z = tiles[3] * scale + wide[0:1, :]
    log_decay = (jnp.minimum(z, 0.0) - jnp.log1p(jnp.exp(-jnp.abs(z)))) / 16.0
    decay = jnp.exp(log_decay)
    decay = jnp.where(low, decay, pltpu.roll(decay, 64, 1))
    right = (lane >= 64).astype(jnp.int32)
    for b in range(64):
        v = jnp.take_along_axis(value, right + 2 * b, axis=1)
        new = decay * old[0, :, b * 128 : b * 128 + 128] + key * v
        new_ref[0, :, b * 128 : b * 128 + 128] = new
        reads[b * LS : b * LS + LS, :] = query * new
    row = lax.broadcasted_iota(jnp.int32, (128, 128), 0)
    col = lax.broadcasted_iota(jnp.int32, (128, 128), 1)
    fold = ((row >= 64) == (col % 2 == 1)).astype(f32).astype(bf16)
    product = reads[...]
    high = product.astype(bf16)
    rest = (product - high.astype(f32)).astype(bf16)
    sums = jnp.dot(high, fold, preferred_element_type=f32) + jnp.dot(rest, fold, preferred_element_type=f32)
    readout = jnp.zeros((LS, 128), f32)
    for b in range(64):
        readout = jnp.where(lane // 2 == b, sums[b * LS : b * LS + LS, :], readout)
    readout = readout * KEY ** (-0.5)
    mean = jnp.sum(readout * readout, axis=1, keepdims=True) / VAL
    silu = gate / (1.0 + jnp.exp(-gate))
    return (readout * lax.rsqrt(mean + epsilon) * gain * silu).astype(bf16)


def shape(s, t=bf16):
    return jax.ShapeDtypeStruct(s, t)


def local(tokens, recurrent_state, pre_gain, w_query, w_key, w_value, w_gate, w_decay, decay_bias, head_gain, w_out, post_gain):
    turned = lambda w: jnp.swapaxes(w, 1, 2)
    weights = (turned(w_query), turned(w_key), w_value, w_gate, turned(w_decay))

    def weight_specs(b):
        return [whole((1, *w.shape[1:]), (b, 0, 0)) for w in weights]

    def exchange(array, axis):
        return lax.all_to_all(array, axis, 0, 0, tiled=True)

    pair = whole((2, 256))
    second_narrow = whole((1, 64, 256), (1, 0, 0))
    scratch = [pltpu.VMEM((8, 128), f32), pltpu.VMEM((64 * LS, 128), f32)]
    out_spec = whole((TP, 8, 256))

    def reduced(mixed, b):
        spread = call(
            first_out_body,
            shape((TP, 8, 256)),
            [whole((DP, LS, 128)), whole((1, 128, 256), (b, 0, 0))],
            out_spec,
        )(mixed, w_out)
        return exchange(spread, "tp")

    pay = call(
        partial_body,
        shape((DP, LS, 512)),
        [whole((256, 256)), pair, *weight_specs(0), second_narrow],
        whole((DP, LS, 512)),
    )(*(pltpu.with_memory_space_constraint(a, pltpu.HBM) for a in (tokens, pre_gain, *weights, weights[4])))
    got = exchange(pay, "dp")
    state, mixed = call(
        first_state_body,
        [shape((2, LS, 8192), f32), shape((DP, LS, 256))],
        [whole((DP, LS, 512)), whole((2, 64)), whole((2, 128)), whole((1, LS, 8192))]
        + [whole((256, 256)), pair, second_narrow, second_narrow],
        [whole((1, LS, 8192)), whole((DP, LS, 256))],
        scratch,
    )(got, decay_bias, head_gain, recurrent_state, tokens, pre_gain, weights[0], weights[1])
    first, mid = got, exchange(mixed, "dp")
    arrived = reduced(mid, 0)
    own0 = call(total_body, shape((TP, 8, 256)), [out_spec], out_spec)(arrived)
    full0 = exchange(own0, "tp")
    pay = call(
        second_partial_body,
        shape((DP, LS, 768)),
        [out_spec, whole((256, 256)), pair, pair, *weight_specs(1)],
        whole((DP, LS, 768)),
    )(full0, tokens, pre_gain, post_gain, *weights)
    got = exchange(pay, "dp")
    state, mixed = call(
        second_state_body,
        [shape((2, LS, 8192), f32), shape((DP, LS, 128))],
        [whole((DP, LS, 768)), whole((DP, LS, 128), (0, 0, 3)), whole((DP, LS, 128), (0, 0, 1))]
        + [whole((2, 64)), whole((2, 128))]
        + [whole((1, LS, 8192), (1, 0, 0)), pl.BlockSpec(memory_space=pl.ANY)],
        [whole((1, LS, 8192), (1, 0, 0)), whole((DP, LS, 128))],
        scratch,
        {6: 0},
    )(got, first, mid, decay_bias, head_gain, recurrent_state, state)
    arrived = reduced(exchange(mixed, "dp"), 1)
    rows = whole((8, 256))
    one = whole((1, 8, 256))
    total, pay = call(
        squares_body,
        [shape((8, 256), f32), shape((DP, 8, 128))],
        [out_spec, one],
        [rows, whole((DP, 8, 128))],
    )(arrived, own0)
    got = exchange(pay, "dp")
    own = call(
        final_body,
        shape((TP, 8, 256)),
        [whole((DP, 8, 128)), rows, one, out_spec, pair],
        out_spec,
    )(got, total, own0, tokens.reshape(TP, 8, 256), post_gain)
    hidden = exchange(own, "tp").reshape(256, 256)
    return (hidden, state)


def solution(mesh):
    in_specs = (
        P(None, "dp"),
        P(None, "dp", "tp"),
        P(None, "dp"),
        P(None, "dp", "tp"),
        P(None, "dp", "tp"),
        P(None, "dp", "tp"),
        P(None, "dp", "tp"),
        P(None, "dp", "tp"),
        P(None, "tp"),
        P(),
        P(None, "tp", "dp"),
        P(None, "dp"),
    )
    out_specs = (P(None, "dp"), P(None, "dp", "tp"))

    return jax.shard_map(local, mesh=mesh, in_specs=in_specs, out_specs=out_specs, check_vma=False)
```

```python
import jax
import jax.numpy as jnp
from jax import lax
from jax.experimental import pallas as pl
from jax.experimental.pallas import tpu as pltpu
from jax.sharding import PartitionSpec as P

D = 4096
KEY = 64
VAL = 128
DP = 16
TP = 32
LS = 16
epsilon = 1e-06
bf16 = jnp.bfloat16
f32 = jnp.float32

def whole(shape, index=None):
    at = index or (0,) * len(shape)
    return pl.BlockSpec(shape, lambda i, at=at: at)


def call(body, out_shape, in_specs, out_specs, scratch=(), aliases=None, limit=16):
    return pl.pallas_call(
        body,
        grid=(1,),
        out_shape=out_shape,
        in_specs=in_specs,
        out_specs=out_specs,
        scratch_shapes=scratch,
        input_output_aliases=aliases or {},
        compiler_params=pltpu.CompilerParams(vmem_limit_bytes=limit * 1024 * 1024),
    )


def columns(wq, wk, wv, wg, wd):
    qk = jnp.concatenate([wq[0], wk[0]], axis=0).astype(f32).T.astype(bf16)
    decay = jnp.concatenate([wd[0].astype(f32), jnp.zeros((64, 256), f32)], axis=0).T.astype(bf16)
    return (qk, wv[0], wg[0], decay)


def split3(value):
    high = value.astype(bf16).astype(f32)
    mid = (value - high).astype(bf16).astype(f32)
    return high, mid, value - high - mid


def place(acc, lane, start, values):
    for i, value in enumerate(values):
        acc = jnp.where(lane == start + i, value, acc)
    return acc


def late_columns(wd):
    return jnp.concatenate([jnp.zeros((64, 256), f32), wd[0].astype(f32)], axis=0).T.astype(bf16)


def turned_columns(wq, wk):
    return jnp.concatenate([wq[0], wk[0]], axis=0).astype(f32).T.astype(bf16)


def partial_body(tokens, pre, wq, wk, wv, wg, wd, wd1, pay):
    x = tokens[...].astype(f32)
    squares = jnp.sum(x * x, axis=1, keepdims=True)
    normed = (x * pre[0:1, :]).astype(bf16)
    lane = lax.broadcasted_iota(jnp.int32, (256, 128), 1)
    for i, w in enumerate(columns(wq, wk, wv, wg, wd)):
        acc = jnp.dot(normed, w, preferred_element_type=f32)
        if i == 3:
            late = (x * pre[1:2, :]).astype(bf16)
            acc = acc + jnp.dot(late, late_columns(wd1), preferred_element_type=f32)
            acc = place(acc, lane, 125, split3(squares))
        pay[:, :, 128 * i : 128 * i + 128] = acc.astype(bf16).reshape(DP, LS, 128)


def summed(came, start):
    total = came[0, :, start : start + 128].astype(f32)
    for d in range(1, DP):
        total = total + came[d, :, start : start + 128].astype(f32)
    return total


def last_three(tile):
    return tile[:, 125:126] + tile[:, 126:127] + tile[:, 127:128]


def first_state_body(got, bias, gain, old, tokens, pre, wq1, wk1, new_ref, pay, *scratch):
    tiles = [summed(got, 128 * i) for i in range(4)]
    m, copies = attend(0, tiles, last_three(tiles[3]), bias[0:1, :], gain[0:1, :], old, new_ref, *scratch)
    late = (tokens[...].astype(f32) * pre[1:2, :]).astype(bf16)
    part = jnp.dot(late, turned_columns(wq1, wk1), preferred_element_type=f32)
    pay[:, :, 128:256] = part.astype(bf16).reshape(DP, LS, 128)
    for d in range(DP):
        pay[d, :, 0:128] = m
    for copy in copies:
        copy.wait()


def first_out_body(mixed, wo, out):
    m = mixed[...].reshape(DP * LS, VAL)
    part = jnp.dot(m, wo[0], preferred_element_type=f32)
    out[...] = part.reshape(TP, 8, 256).astype(bf16)


def total_body(arrived, out):
    total = arrived[0].astype(f32)
    for t in range(1, TP):
        total = total + arrived[t].astype(f32)
    total = total.astype(bf16)
    for t in range(TP):
        out[t] = total


def second_partial_body(full, tokens, pre, post, wq, wk, wv, wg, wd, pay):
    x = tokens[...].astype(f32)
    out = full[...].astype(f32).reshape(256, 256)
    step = out * post[0:1, :]
    stats = []
    for value in (out * out, x * step, step * step):
        stats += split3(jnp.sum(value, axis=1, keepdims=True))
    gain = pre[1:2, :]
    lhs, late = (step * gain).astype(bf16), (x * gain).astype(bf16)
    lane = lax.broadcasted_iota(jnp.int32, (256, 128), 1)
    tiles = columns(wq, wk, wv, wg, wd)
    results = [jnp.dot(lhs, w, preferred_element_type=f32) for w in tiles]
    ends = jnp.dot(late, late_columns(wd), preferred_element_type=f32)
    results[3] = place(jnp.where(lane >= 125, ends, results[3]), lane, 64, stats)
    results += [jnp.dot(late, w, preferred_element_type=f32) for w in tiles[1:3]]
    for i, acc in enumerate(results):
        pay[:, :, 128 * i : 128 * i + 128] = acc.astype(bf16).reshape(DP, LS, 128)


def second_state_body(got, first, mid, bias, gain, old, kept, new_ref, mixed, *scratch):
    step = [summed(got, 128 * i) for i in range(4)]
    early = summed(first, 0)
    stats = []
    for i in range(3):
        at = 64 + 3 * i
        stats.append(step[3][:, at : at + 1] + step[3][:, at + 1 : at + 2] + step[3][:, at + 2 : at + 3])
    scale = lax.rsqrt(stats[0] / D + epsilon)
    squares = last_three(early) + 2.0 * scale * stats[1] + scale * scale * stats[2]
    lane = lax.broadcasted_iota(jnp.int32, (LS, 128), 1)
    decay = pltpu.roll(jnp.where(lane >= 125, step[3], early), 64, 1)
    base = [summed(mid, 0), summed(got, 512), summed(got, 640), decay]
    tiles = [x + scale * b for x, b in zip(base, step)]
    m, copies = attend(1, tiles, jnp.maximum(squares, 0.0), bias[1:2, :], gain[1:2, :], old, new_ref, *scratch)
    for d in range(DP):
        mixed[d] = m
    for copy in copies:
        copy.wait()


def squares_body(arrived, own0, total, pay):
    out = arrived[0].astype(f32)
    for t in range(1, TP):
        out = out + arrived[t].astype(f32)
    total[...] = out
    before = own0[0].astype(f32)
    lane = lax.broadcasted_iota(jnp.int32, (8, 128), 1)
    parts = []
    for value in (out, before):
        parts += split3(jnp.sum(value * value, axis=1, keepdims=True))
    acc = place(jnp.zeros((8, 128), f32), lane, 0, parts).astype(bf16)
    for d in range(DP):
        pay[d] = acc


def final_body(got, total, own0, tokens, post, out):
    came = got[0].astype(f32)
    for d in range(1, DP):
        came = came + got[d].astype(f32)
    rates = []
    for i in range(2):
        squares = came[:, 3 * i : 3 * i + 1] + came[:, 3 * i + 1 : 3 * i + 2] + came[:, 3 * i + 2 : 3 * i + 3]
        rates.append(lax.rsqrt(squares / D + epsilon))
    x = tokens[lax.axis_index("tp")].astype(f32)
    x = (x + own0[0].astype(f32) * rates[1] * post[0:1, :]).astype(bf16).astype(f32)
    x = (x + total[...] * rates[0] * post[1:2, :]).astype(bf16)
    for t in range(TP):
        out[t] = x


def attend(block, tiles, squares, bias, gain, old, out, wide, reads, fresh, sems):
    scale = lax.rsqrt(squares / D + epsilon)
    lane = lax.broadcasted_iota(jnp.int32, (LS, 128), 1)
    low = lane < 64
    qk = (tiles[0] * scale).astype(bf16).astype(f32)
    kq = pltpu.roll(qk, 64, 1)
    query = jnp.where(low, qk, kq)
    key = jnp.where(low, kq, qk)
    value = tiles[1] * scale
    gate = tiles[2] * scale
    wide[0:1, 0:64] = bias
    wide[0:1, 64:128] = jnp.zeros((1, 64), f32)
    z = tiles[3] * scale + wide[0:1, :]
    log_decay = (jnp.minimum(z, 0.0) - jnp.log1p(jnp.exp(-jnp.abs(z)))) / 16.0
    decay = jnp.exp(log_decay)
    decay = jnp.where(low, decay, pltpu.roll(decay, 64, 1))
    right = (lane >= 64).astype(jnp.int32)
    copies = []
    for b in range(64):
        v = jnp.take_along_axis(value, right + 2 * b, axis=1)
        new = decay * old[0, :, b * 128 : b * 128 + 128] + key * v
        fresh[:, b * 128 : b * 128 + 128] = new
        reads[b * LS : b * LS + LS, :] = query * new
        if b % 16 == 15:
            at = pl.ds((b // 16) * 2048, 2048)
            copy = pltpu.make_async_copy(fresh.at[:, at], out.at[block, :, at], sems.at[b // 16])
            copy.start()
            copies.append(copy)
    row = lax.broadcasted_iota(jnp.int32, (128, 128), 0)
    col = lax.broadcasted_iota(jnp.int32, (128, 128), 1)
    fold = ((row >= 64) == (col % 2 == 1)).astype(f32).astype(bf16)
    product = reads[...]
    high = product.astype(bf16)
    rest = (product - high.astype(f32)).astype(bf16)
    sums = jnp.dot(high, fold, preferred_element_type=f32) + jnp.dot(rest, fold, preferred_element_type=f32)
    readout = jnp.zeros((LS, 128), f32)
    for b in range(64):
        readout = jnp.where(lane // 2 == b, sums[b * LS : b * LS + LS, :], readout)
    readout = readout * KEY ** (-0.5)
    mean = jnp.sum(readout * readout, axis=1, keepdims=True) / VAL
    silu = gate / (1.0 + jnp.exp(-gate))
    return (readout * lax.rsqrt(mean + epsilon) * gain * silu).astype(bf16), copies


def shape(s, t=bf16):
    return jax.ShapeDtypeStruct(s, t)


def local(tokens, recurrent_state, pre_gain, w_query, w_key, w_value, w_gate, w_decay, decay_bias, head_gain, w_out, post_gain):
    turned = lambda w: jnp.swapaxes(w, 1, 2)
    weights = (turned(w_query), turned(w_key), w_value, w_gate, turned(w_decay))

    def weight_specs(b):
        return [whole((1, *w.shape[1:]), (b, 0, 0)) for w in weights]

    def exchange(array, axis):
        return lax.all_to_all(array, axis, 0, 0, tiled=True)

    pair = whole((2, 256))
    second_narrow = whole((1, 64, 256), (1, 0, 0))
    scratch = [
        pltpu.VMEM((8, 128), f32),
        pltpu.VMEM((64 * LS, 128), f32),
        pltpu.VMEM((LS, 8192), f32),
        pltpu.SemaphoreType.DMA((4,)),
    ]
    anywhere = pl.BlockSpec(memory_space=pl.ANY)
    out_spec = whole((TP, 8, 256))

    def reduced(mixed, b):
        spread = call(
            first_out_body,
            shape((TP, 8, 256)),
            [whole((DP, LS, 128)), whole((1, 128, 256), (b, 0, 0))],
            out_spec,
        )(mixed, w_out)
        return exchange(spread, "tp")

    pay = call(
        partial_body,
        shape((DP, LS, 512)),
        [whole((256, 256)), pair, *weight_specs(0), second_narrow],
        whole((DP, LS, 512)),
    )(*(pltpu.with_memory_space_constraint(a, pltpu.HBM) for a in (tokens, pre_gain, *weights, weights[4])))
    got = exchange(pay, "dp")
    state, mixed = call(
        first_state_body,
        [shape((2, LS, 8192), f32), shape((DP, LS, 256))],
        [whole((DP, LS, 512)), whole((2, 64)), whole((2, 128)), whole((1, LS, 8192))]
        + [whole((256, 256)), pair, second_narrow, second_narrow],
        [anywhere, whole((DP, LS, 256))],
        scratch,
    )(got, decay_bias, head_gain, recurrent_state, tokens, pre_gain, weights[0], weights[1])
    first, mid = got, exchange(mixed, "dp")
    arrived = reduced(mid, 0)
    own0 = call(total_body, shape((TP, 8, 256)), [out_spec], out_spec)(arrived)
    full0 = exchange(own0, "tp")
    pay = call(
        second_partial_body,
        shape((DP, LS, 768)),
        [out_spec, whole((256, 256)), pair, pair, *weight_specs(1)],
        whole((DP, LS, 768)),
    )(full0, tokens, pre_gain, post_gain, *weights)
    got = exchange(pay, "dp")
    state, mixed = call(
        second_state_body,
        [shape((2, LS, 8192), f32), shape((DP, LS, 128))],
        [whole((DP, LS, 768)), whole((DP, LS, 128), (0, 0, 3)), whole((DP, LS, 128), (0, 0, 1))]
        + [whole((2, 64)), whole((2, 128))]
        + [whole((1, LS, 8192), (1, 0, 0)), anywhere],
        [anywhere, whole((DP, LS, 128))],
        scratch,
        {6: 0},
    )(got, first, mid, decay_bias, head_gain, recurrent_state, state)
    arrived = reduced(exchange(mixed, "dp"), 1)
    rows = whole((8, 256))
    one = whole((1, 8, 256))
    total, pay = call(
        squares_body,
        [shape((8, 256), f32), shape((DP, 8, 128))],
        [out_spec, one],
        [rows, whole((DP, 8, 128))],
    )(arrived, own0)
    got = exchange(pay, "dp")
    own = call(
        final_body,
        shape((TP, 8, 256)),
        [whole((DP, 8, 128)), rows, one, out_spec, pair],
        out_spec,
    )(got, total, own0, tokens.reshape(TP, 8, 256), post_gain)
    hidden = exchange(own, "tp").reshape(256, 256)
    return (hidden, state)


def solution(mesh):
    in_specs = (
        P(None, "dp"),
        P(None, "dp", "tp"),
        P(None, "dp"),
        P(None, "dp", "tp"),
        P(None, "dp", "tp"),
        P(None, "dp", "tp"),
        P(None, "dp", "tp"),
        P(None, "dp", "tp"),
        P(None, "tp"),
        P(),
        P(None, "tp", "dp"),
        P(None, "dp"),
    )
    out_specs = (P(None, "dp"), P(None, "dp", "tp"))

    return jax.shard_map(local, mesh=mesh, in_specs=in_specs, out_specs=out_specs, check_vma=False)
```

```python
import jax
import jax.numpy as jnp
from jax import lax
from jax.experimental import pallas as pl
from jax.experimental.pallas import tpu as pltpu
from jax.sharding import PartitionSpec as P

D = 4096
KEY = 64
VAL = 128
DP = 16
TP = 32
LS = 16
epsilon = 1e-06
bf16 = jnp.bfloat16
f32 = jnp.float32

def whole(shape, index=None):
    at = index or (0,) * len(shape)
    return pl.BlockSpec(shape, lambda i, at=at: at)


def call(body, out_shape, in_specs, out_specs, scratch=(), aliases=None, limit=16):
    return pl.pallas_call(
        body,
        grid=(1,),
        out_shape=out_shape,
        in_specs=in_specs,
        out_specs=out_specs,
        scratch_shapes=scratch,
        input_output_aliases=aliases or {},
        compiler_params=pltpu.CompilerParams(vmem_limit_bytes=limit * 1024 * 1024),
    )


def columns(wq, wk, wv, wg, wd):
    qk = jnp.concatenate([wq[0], wk[0]], axis=0).astype(f32).T.astype(bf16)
    decay = jnp.concatenate([wd[0].astype(f32), jnp.zeros((64, 256), f32)], axis=0).T.astype(bf16)
    return (qk, wv[0], wg[0], decay)


def split3(value):
    high = value.astype(bf16).astype(f32)
    mid = (value - high).astype(bf16).astype(f32)
    return high, mid, value - high - mid


def place(acc, lane, start, values):
    for i, value in enumerate(values):
        acc = jnp.where(lane == start + i, value, acc)
    return acc


def late_columns(wd):
    return jnp.concatenate([jnp.zeros((64, 256), f32), wd[0].astype(f32)], axis=0).T.astype(bf16)


def turned_columns(wq, wk):
    return jnp.concatenate([wq[0], wk[0]], axis=0).astype(f32).T.astype(bf16)


def partial_body(tokens, pre, wq, wk, wv, wg, wd, wd1, pay):
    x = tokens[...].astype(f32)
    squares = jnp.sum(x * x, axis=1, keepdims=True)
    normed = (x * pre[0:1, :]).astype(bf16)
    lane = lax.broadcasted_iota(jnp.int32, (256, 128), 1)
    for i, w in enumerate(columns(wq, wk, wv, wg, wd)):
        acc = jnp.dot(normed, w, preferred_element_type=f32)
        if i == 3:
            late = (x * pre[1:2, :]).astype(bf16)
            acc = acc + jnp.dot(late, late_columns(wd1), preferred_element_type=f32)
            acc = place(acc, lane, 125, split3(squares))
        pay[:, :, 128 * i : 128 * i + 128] = acc.astype(bf16).reshape(DP, LS, 128)


def summed(came, start):
    total = came[0, :, start : start + 128].astype(f32)
    for d in range(1, DP):
        total = total + came[d, :, start : start + 128].astype(f32)
    return total


def last_three(tile):
    return tile[:, 125:126] + tile[:, 126:127] + tile[:, 127:128]


def first_state_body(got, bias, gain, old, tokens, pre, wq1, wk1, new_ref, pay, *scratch):
    tiles = [summed(got, 128 * i) for i in range(4)]
    m, copies = attend(0, tiles, last_three(tiles[3]), bias[0:1, :], gain[0:1, :], old, new_ref, *scratch)
    late = (tokens[...].astype(f32) * pre[1:2, :]).astype(bf16)
    part = jnp.dot(late, turned_columns(wq1, wk1), preferred_element_type=f32)
    pay[:, :, 128:256] = part.astype(bf16).reshape(DP, LS, 128)
    for d in range(DP):
        pay[d, :, 0:128] = m
    for copy in copies:
        copy.wait()


def first_out_body(mixed, wo, out):
    m = mixed[...].reshape(DP * LS, VAL)
    part = jnp.dot(m, wo[0], preferred_element_type=f32)
    out[...] = part.reshape(TP, 8, 256).astype(bf16)


def total_body(arrived, out):
    total = arrived[0].astype(f32)
    for t in range(1, TP):
        total = total + arrived[t].astype(f32)
    total = total.astype(bf16)
    for t in range(TP):
        out[t] = total


def second_partial_body(full, tokens, pre, post, wq, wk, wv, wg, wd, pay):
    x = tokens[...].astype(f32)
    out = full[...].astype(f32).reshape(256, 256)
    step = out * post[0:1, :]
    stats = []
    for value in (out * out, x * step, step * step):
        stats += split3(jnp.sum(value, axis=1, keepdims=True))
    gain = pre[1:2, :]
    lhs, late = (step * gain).astype(bf16), (x * gain).astype(bf16)
    lane = lax.broadcasted_iota(jnp.int32, (256, 128), 1)
    tiles = columns(wq, wk, wv, wg, wd)
    results = [jnp.dot(lhs, w, preferred_element_type=f32) for w in tiles]
    ends = jnp.dot(late, late_columns(wd), preferred_element_type=f32)
    results[3] = place(jnp.where(lane >= 125, ends, results[3]), lane, 64, stats)
    results += [jnp.dot(late, w, preferred_element_type=f32) for w in tiles[1:3]]
    for i, acc in enumerate(results):
        pay[:, :, 128 * i : 128 * i + 128] = acc.astype(bf16).reshape(DP, LS, 128)


def second_state_body(got, first, mid, bias, gain, old, kept, new_ref, mixed, *scratch):
    step = [summed(got, 128 * i) for i in range(4)]
    early = summed(first, 0)
    stats = []
    for i in range(3):
        at = 64 + 3 * i
        stats.append(step[3][:, at : at + 1] + step[3][:, at + 1 : at + 2] + step[3][:, at + 2 : at + 3])
    scale = lax.rsqrt(stats[0] / D + epsilon)
    squares = last_three(early) + 2.0 * scale * stats[1] + scale * scale * stats[2]
    lane = lax.broadcasted_iota(jnp.int32, (LS, 128), 1)
    decay = pltpu.roll(jnp.where(lane >= 125, step[3], early), 64, 1)
    base = [summed(mid, 0), summed(got, 512), summed(got, 640), decay]
    tiles = [x + scale * b for x, b in zip(base, step)]
    m, copies = attend(1, tiles, jnp.maximum(squares, 0.0), bias[1:2, :], gain[1:2, :], old, new_ref, *scratch)
    for d in range(DP):
        mixed[d] = m
    for copy in copies:
        copy.wait()


def squares_body(arrived, own0, total, pay):
    out = arrived[0].astype(f32)
    for t in range(1, TP):
        out = out + arrived[t].astype(f32)
    total[...] = out
    before = own0[0].astype(f32)
    lane = lax.broadcasted_iota(jnp.int32, (8, 128), 1)
    parts = []
    for value in (out, before):
        parts += split3(jnp.sum(value * value, axis=1, keepdims=True))
    acc = place(jnp.zeros((8, 128), f32), lane, 0, parts).astype(bf16)
    for d in range(DP):
        pay[d] = acc


def final_body(got, total, own0, tokens, post, out):
    came = got[0].astype(f32)
    for d in range(1, DP):
        came = came + got[d].astype(f32)
    rates = []
    for i in range(2):
        squares = came[:, 3 * i : 3 * i + 1] + came[:, 3 * i + 1 : 3 * i + 2] + came[:, 3 * i + 2 : 3 * i + 3]
        rates.append(lax.rsqrt(squares / D + epsilon))
    x = tokens[lax.axis_index("tp")].astype(f32)
    x = (x + own0[0].astype(f32) * rates[1] * post[0:1, :]).astype(bf16).astype(f32)
    x = (x + total[...] * rates[0] * post[1:2, :]).astype(bf16)
    for t in range(TP):
        out[t] = x


def attend(block, tiles, squares, bias, gain, old, out, wide, reads, fresh, sems):
    scale = lax.rsqrt(squares / D + epsilon)
    lane = lax.broadcasted_iota(jnp.int32, (LS, 128), 1)
    low = lane < 64
    qk = (tiles[0] * scale).astype(bf16).astype(f32)
    kq = pltpu.roll(qk, 64, 1)
    query = jnp.where(low, qk, kq)
    key = jnp.where(low, kq, qk)
    value = tiles[1] * scale
    gate = tiles[2] * scale
    wide[0:1, 0:64] = bias
    wide[0:1, 64:128] = jnp.zeros((1, 64), f32)
    z = tiles[3] * scale + wide[0:1, :]
    log_decay = (jnp.minimum(z, 0.0) - jnp.log1p(jnp.exp(-jnp.abs(z)))) / 16.0
    decay = jnp.exp(log_decay)
    decay = jnp.where(low, decay, pltpu.roll(decay, 64, 1))
    right = (lane >= 64).astype(jnp.int32)
    copies = []
    for b in range(64):
        v = jnp.take_along_axis(value, right + 2 * b, axis=1)
        new = decay * old[0, :, b * 128 : b * 128 + 128] + key * v
        fresh[:, b * 128 : b * 128 + 128] = new
        reads[b * LS : b * LS + LS, :] = (query * new).astype(bf16)
        if b % 8 == 7:
            at = pl.ds((b // 8) * 1024, 1024)
            copy = pltpu.make_async_copy(fresh.at[:, at], out.at[block, :, at], sems.at[b // 8])
            copy.start()
            copies.append(copy)
    row = lax.broadcasted_iota(jnp.int32, (128, 128), 0)
    col = lax.broadcasted_iota(jnp.int32, (128, 128), 1)
    fold = ((row >= 64) == (col % 2 == 1)).astype(f32).astype(bf16)
    sums = jnp.dot(reads[...], fold, preferred_element_type=f32)
    readout = jnp.zeros((LS, 128), f32)
    for b in range(64):
        readout = jnp.where(lane // 2 == b, sums[b * LS : b * LS + LS, :], readout)
    readout = readout * KEY ** (-0.5)
    mean = jnp.sum(readout * readout, axis=1, keepdims=True) / VAL
    silu = gate / (1.0 + jnp.exp(-gate))
    return (readout * lax.rsqrt(mean + epsilon) * gain * silu).astype(bf16), copies


def shape(s, t=bf16):
    return jax.ShapeDtypeStruct(s, t)


def local(tokens, recurrent_state, pre_gain, w_query, w_key, w_value, w_gate, w_decay, decay_bias, head_gain, w_out, post_gain):
    turned = lambda w: jnp.swapaxes(w, 1, 2)
    weights = (turned(w_query), turned(w_key), w_value, w_gate, turned(w_decay))

    def weight_specs(b):
        return [whole((1, *w.shape[1:]), (b, 0, 0)) for w in weights]

    def exchange(array, axis):
        return lax.all_to_all(array, axis, 0, 0, tiled=True)

    pair = whole((2, 256))
    second_narrow = whole((1, 64, 256), (1, 0, 0))
    scratch = [
        pltpu.VMEM((8, 128), f32),
        pltpu.VMEM((64 * LS, 128), bf16),
        pltpu.VMEM((LS, 8192), f32),
        pltpu.SemaphoreType.DMA((8,)),
    ]
    anywhere = pl.BlockSpec(memory_space=pl.ANY)
    out_spec = whole((TP, 8, 256))

    def reduced(mixed, b):
        spread = call(
            first_out_body,
            shape((TP, 8, 256)),
            [whole((DP, LS, 128)), whole((1, 128, 256), (b, 0, 0))],
            out_spec,
        )(mixed, w_out)
        return exchange(spread, "tp")

    pay = call(
        partial_body,
        shape((DP, LS, 512)),
        [whole((256, 256)), pair, *weight_specs(0), second_narrow],
        whole((DP, LS, 512)),
    )(*(pltpu.with_memory_space_constraint(a, pltpu.HBM) for a in (tokens, pre_gain, *weights, weights[4])))
    got = exchange(pay, "dp")
    state, mixed = call(
        first_state_body,
        [shape((2, LS, 8192), f32), shape((DP, LS, 256))],
        [whole((DP, LS, 512)), whole((2, 64)), whole((2, 128)), whole((1, LS, 8192))]
        + [whole((256, 256)), pair, second_narrow, second_narrow],
        [anywhere, whole((DP, LS, 256))],
        scratch,
    )(got, decay_bias, head_gain, recurrent_state, tokens, pre_gain, weights[0], weights[1])
    first, mid = got, exchange(mixed, "dp")
    arrived = reduced(mid, 0)
    own0 = call(total_body, shape((TP, 8, 256)), [out_spec], out_spec)(arrived)
    full0 = exchange(own0, "tp")
    pay = call(
        second_partial_body,
        shape((DP, LS, 768)),
        [out_spec, whole((256, 256)), pair, pair, *weight_specs(1)],
        whole((DP, LS, 768)),
    )(full0, tokens, pre_gain, post_gain, *weights)
    got = exchange(pay, "dp")
    state, mixed = call(
        second_state_body,
        [shape((2, LS, 8192), f32), shape((DP, LS, 128))],
        [whole((DP, LS, 768)), whole((DP, LS, 128), (0, 0, 3)), whole((DP, LS, 128), (0, 0, 1))]
        + [whole((2, 64)), whole((2, 128))]
        + [whole((1, LS, 8192), (1, 0, 0)), anywhere],
        [anywhere, whole((DP, LS, 128))],
        scratch,
        {6: 0},
    )(got, first, mid, decay_bias, head_gain, recurrent_state, state)
    arrived = reduced(exchange(mixed, "dp"), 1)
    rows = whole((8, 256))
    one = whole((1, 8, 256))
    total, pay = call(
        squares_body,
        [shape((8, 256), f32), shape((DP, 8, 128))],
        [out_spec, one],
        [rows, whole((DP, 8, 128))],
    )(arrived, own0)
    got = exchange(pay, "dp")
    own = call(
        final_body,
        shape((TP, 8, 256)),
        [whole((DP, 8, 128)), rows, one, out_spec, pair],
        out_spec,
    )(got, total, own0, tokens.reshape(TP, 8, 256), post_gain)
    hidden = exchange(own, "tp").reshape(256, 256)
    return (hidden, state)


def solution(mesh):
    in_specs = (
        P(None, "dp"),
        P(None, "dp", "tp"),
        P(None, "dp"),
        P(None, "dp", "tp"),
        P(None, "dp", "tp"),
        P(None, "dp", "tp"),
        P(None, "dp", "tp"),
        P(None, "dp", "tp"),
        P(None, "tp"),
        P(),
        P(None, "tp", "dp"),
        P(None, "dp"),
    )
    out_specs = (P(None, "dp"), P(None, "dp", "tp"))

    return jax.shard_map(local, mesh=mesh, in_specs=in_specs, out_specs=out_specs, check_vma=False)
```
